32 devices in a mesh: grp: 2 (over y), fs: 4 (over z), tp: 4 (over x, core).
Axes of the slice: x: 2, y: 2, z: 4, core: 2. Of those that a mesh axis runs over, the one named last changes fastest.
Arguments:
- tokens: bfloat16 [2048, 2048], P(('grp', 'fs')), parts along dimension 0, may hold values from -6 to 6
- norm_gain: float32 [2048], P('fs'), may hold values from 0.1 to 1.9
- gate_master: float32 [4, 2048, 1024], P(None, 'fs', 'tp'), may hold values from -0.125 to 0.125
- up_master: float32 [4, 2048, 1024], P(None, 'fs', 'tp'), may hold values from -0.125 to 0.125
- chosen: int32 [2048, 2], P(('grp', 'fs')), parts along dimension 0, may hold values from 0 to 3, all different within a row; in each aligned block of 256 rows (0 to 255, 256 to 511, ...) at most 256 rows name the same one
- affinity: float32 [2048, 2], P(('grp', 'fs')), parts along dimension 0, may hold values from 0.05 to 1
Outputs:
- gate_served: bfloat16 [8, 2048, 1024], P(('grp', 'fs'), None, 'tp'), parts along dimension 0
- up_served: bfloat16 [8, 2048, 1024], P(('grp', 'fs'), None, 'tp'), parts along dimension 0
- hidden: bfloat16 [2048, 2, 1024], P(('grp', 'fs'), None, 'tp'), parts along dimension 0
The draws below stay inside these ranges and needn't reach their ends.
There are 2 independent parts, one for each index of `grp`. The reference program is written for one: setup_inputs(seed, part) draws one part's arguments, and reference() takes and returns one part's arrays. A program takes and returns all parts, laid end to end along the dimension named above; an argument that names none is the same for every part. Nothing has to cross between parts.
Inputs may be any that keep to these rules, and one draw needn't show every extreme that they name: Among the rows of one index of fs (256 tokens, all their choices) no expert is chosen more than 256 times, a bound that some block reaches; the choices of one token differ.
All inputs are finite; a program needn't handle non-finite values.
Results may differ from the reference program's by a relative error of at most 0.023.
Values may be sent and summed in bfloat16 or wider, within the bound.
A program may use at most 64 MiB of HBM per device.

```python
import math
import jax
import jax.numpy as jnp
import numpy as np
from jax import lax

D = 2048
F = 1024
TOP = 2
TOK_DEV = 256
EXPERTS = 4
TOKENS = 1024
CAP = 256
N_FS = 4


def levels(key, dims, shards, least, largest):
    loudness, own = 1.0, jax.random.fold_in(key, 6)
    for axis_at, blocks in shards:
        draws = jnp.exp(jax.random.uniform(jax.random.fold_in(own, axis_at), (blocks,), jnp.float32, least / len(shards), largest / len(shards)))
        loudness = loudness * jnp.repeat(draws, dims[axis_at] // blocks).reshape([-1 if axis == axis_at else 1 for axis in range(len(dims))])
    return loudness


def assign_block(rng, own, number, rows, amount, top, limit, lean):
    ranking = jax.random.permutation(rng, amount)
    crowded, ordinary = shares(amount, rows * top, limit, lean, True), shares(amount, rows * top, limit, lean, False)
    places = jnp.arange(amount)

    def named(tallies, turn):
        used = int((tallies > 0).sum())
        fixed = max(1, used // 4)
        passed = fixed + (places - fixed + turn * (used - fixed)) % max(1, amount - fixed)
        return jnp.zeros((amount,), jnp.int32).at[ranking[jnp.where(places < fixed, places, passed)]].set(jnp.asarray(tallies, jnp.int32))

    tallies = jnp.where(number % 4 == 0, named(crowded, number // 4), named(ordinary, number - number // 4 - 1))
    mixed = jax.random.permutation(jax.random.fold_in(own, 3), amount)
    giver, sink = mixed[0:amount // 2 * 2:2], mixed[1:amount // 2 * 2:2]
    slack = jnp.minimum(tallies[giver] - 1, limit - tallies[sink]) // 2
    slack = jnp.where((giver == ranking[0]) | (sink == ranking[0]) | (tallies[sink] == 0), 0, jnp.maximum(slack, 0))
    passed = jax.random.randint(jax.random.fold_in(own, 4), (amount // 2,), 0, 1 << 20) % (slack + 1)
    tallies = tallies.at[giver].add(-passed).at[sink].add(passed)
    members = jnp.searchsorted(jnp.cumsum(tallies), jnp.arange(rows * top), side="right").astype(jnp.int32)
    table = members.reshape(top, rows).T
    table = table[jax.random.permutation(jax.random.fold_in(own, 1), rows)]
    turn = jax.random.randint(jax.random.fold_in(own, 2), (rows, 1), 0, top)
    return jnp.take_along_axis(table, (jnp.arange(top)[None, :] + turn) % top, axis=1)


def shares(amount, total, most, lean, full):
    weights = [(1 << 20) // math.isqrt(grade ** lean) + 1 for grade in range(1, amount + 1)]
    largest = most if full else min(most, max(-(-total // amount), total * weights[0] // sum(weights)))
    least = 1 if total - largest >= amount - 1 else 0
    counts, rest = [largest] + [least] * (amount - 1), total - largest - least * (amount - 1)
    while rest > 0:
        candidates = [i for i in range(1, amount) if counts[i] < largest] or [i for i in range(1, amount) if counts[i] < most]
        pool, budget = sum([weights[i] for i in candidates]), rest
        for i in candidates:
            extra = min(most - counts[i], max(1, budget * weights[i] // pool), rest)
            counts[i] = counts[i] + extra
            rest = rest - extra
    return np.array(counts)


def bell_draw(own_key, shape, spread, most, split=(), kind=jnp.bfloat16):
    factor_of = levels(own_key, shape, split, -0.22, 0.18) if split else 1.0
    result = jax.random.normal(own_key, shape, jnp.float32) * spread * factor_of
    return jnp.minimum(jnp.maximum(result, -most), most).astype(kind)


def setup_inputs(seed: int = 0, part: int = 0) -> dict:
    key_of = jax.random.split(jax.random.key(seed), 7)
    part_splits = jax.random.split(jax.random.fold_in(key_of[6], part), 7)
    tokens = bell_draw(part_splits[0], (TOKENS, D), 1.0, 6.0, ((0, 4),))
    norm_gain = jnp.clip(1.0 + 0.18 * jax.random.normal(key_of[1], (D,), jnp.float32), 0.1, 1.9)
    gate_master = bell_draw(key_of[2], (EXPERTS, D, F), D ** -0.5, 0.125, ((1, 4), (2, 4)), jnp.float32)
    up_master = bell_draw(key_of[3], (EXPERTS, D, F), D ** -0.5, 0.125, ((1, 4), (2, 4)), jnp.float32)
    chosen_keys = jax.random.split(jax.random.fold_in(part_splits[4], 1), TOKENS // TOK_DEV)
    chosen_turns = jax.random.permutation(jax.random.fold_in(part_splits[4], 3), TOKENS // TOK_DEV)
    chosen = jax.vmap(lambda own, number: assign_block(jax.random.fold_in(part_splits[4], 2), own, number, TOK_DEV, EXPERTS, TOP, CAP, 2))(chosen_keys, chosen_turns).reshape((TOKENS, TOP))
    affinity = jnp.clip(jnp.exp(math.log(1.0) - 2.9957323 * jax.random.uniform(part_splits[5], (TOKENS, TOP), jnp.float32) ** levels(part_splits[5], (TOKENS, TOP), ((0, 4),), -0.2, 0.2)), 0.05, 1.0)
    return {"tokens": tokens, "norm_gain": norm_gain, "gate_master": gate_master, "up_master": up_master, "chosen": chosen, "affinity": affinity}


def reference(tokens, norm_gain, gate_master, up_master, chosen, affinity):
    gate_served = (gate_master * norm_gain[None, :, None]).astype(jnp.bfloat16)
    up_served = (up_master * norm_gain[None, :, None]).astype(jnp.bfloat16)
    xfloat = tokens.astype(jnp.float32)
    scale = lax.rsqrt(lax.optimization_barrier(jnp.mean(xfloat * xfloat, axis=-1)) + 1e-06)
    share = affinity / lax.optimization_barrier(jnp.sum(affinity, axis=-1, keepdims=True))
    blocks = chosen.reshape(N_FS, TOK_DEV * TOP)
    onehot = (blocks[:, :, None] == jnp.arange(EXPERTS, dtype=jnp.int32)[None, None, :]).astype(jnp.int32)
    slot = lax.optimization_barrier(jnp.sum((jnp.cumsum(onehot, axis=1) - onehot) * onehot, axis=2)).astype(jnp.int32)
    source = jnp.arange(N_FS, dtype=jnp.int32)[:, None]
    column = (source * CAP + slot).reshape(-1).astype(jnp.int32)
    owner = (source * TOK_DEV + jnp.repeat(jnp.arange(TOK_DEV, dtype=jnp.int32), TOP)[None, :]).reshape(-1).astype(jnp.int32)
    flat_e = blocks.reshape(-1).astype(jnp.int32)
    index_buf = jnp.zeros((EXPERTS, N_FS * CAP), jnp.int32).at[flat_e, column].set(owner)
    share_buf = jnp.zeros((EXPERTS, N_FS * CAP), jnp.float32).at[flat_e, column].set(share.reshape(-1))

    def one_expert(args):
        index, weight, w_gate, w_up = args
        rows = tokens[index]
        factor = scale[index][:, None]
        gate = jnp.dot(rows, w_gate, preferred_element_type=jnp.float32) * factor
        up = jnp.dot(rows, w_up, preferred_element_type=jnp.float32) * factor
        return (weight[:, None] * jax.nn.silu(gate) * up).astype(jnp.bfloat16)
    hidden_buf = lax.map(one_expert, (index_buf, share_buf, gate_served, up_served))
    hidden = hidden_buf[flat_e, column].reshape(TOKENS, TOP, F)
    return (gate_served, up_served, hidden)
```

```python
import functools

import jax
import jax.numpy as jnp
from jax import lax
from jax.experimental import pallas as pl
from jax.experimental.pallas import tpu as pltpu
from jax.sharding import PartitionSpec as P

MESH = pl.DeviceIdType.MESH
CHUNKS = 2
HALVES = 2


def routed(tokens, norm_gain, gate_master, up_master, chosen, affinity):
    folded_gate = (gate_master * norm_gain[None, :, None]).astype(jnp.bfloat16)
    folded_up = (up_master * norm_gain[None, :, None]).astype(jnp.bfloat16)
    new_gate, new_up = (
        lax.all_to_all(folded_gate, "fs", split_axis=0, concat_axis=1, tiled=True),
        lax.all_to_all(folded_up, "fs", split_axis=0, concat_axis=1, tiled=True),
    )
    experts_all = gate_master.shape[0]
    tok_rows, width = tokens.shape
    top = chosen.shape[1]
    capacity = tok_rows * top * 2 // experts_all
    local = new_gate.shape[0]
    xfloat = tokens.astype(jnp.float32)
    scale = lax.rsqrt(jnp.mean(xfloat * xfloat, axis=-1) + 1e-06)
    share = affinity / jnp.sum(affinity, axis=-1, keepdims=True)
    flat_e = chosen.reshape(-1)
    onehot = (flat_e[:, None] == jnp.arange(experts_all, dtype=jnp.int32)[None, :]).astype(
        jnp.int32
    )
    slot = jnp.sum((jnp.cumsum(onehot, axis=0) - onehot) * onehot, axis=1)
    target = flat_e * capacity + slot
    owner = jnp.repeat(jnp.arange(tok_rows, dtype=jnp.int32), top)
    total = experts_all * capacity
    scale_buf = (
        jnp.zeros((total,), jnp.float32).at[target].set(scale[owner]).reshape(experts_all, capacity)
    )
    share_buf = (
        jnp.zeros((total,), jnp.float32)
        .at[target]
        .set(share.reshape(-1))
        .reshape(experts_all, capacity)
    )
    narrow = width // lax.axis_size("tp")
    own_cols = lax.dynamic_slice_in_dim(tokens, lax.axis_index("tp") * narrow, narrow, 1)
    row_buf = jnp.zeros((total, narrow), jnp.bfloat16).at[target].set(own_cols[owner])
    row_buf = row_buf.reshape(experts_all, capacity, narrow)
    got_rows, got_scale, got_share = (
        lax.all_to_all(row_buf, "fs", split_axis=0, concat_axis=0, tiled=True),
        lax.all_to_all(
            scale_buf.astype(jnp.bfloat16), "fs", split_axis=0, concat_axis=0, tiled=True
        ).astype(scale_buf.dtype),
        lax.all_to_all(
            share_buf.astype(jnp.bfloat16), "fs", split_axis=0, concat_axis=0, tiled=True
        ).astype(share_buf.dtype),
    )
    sources = got_rows.shape[0] // local
    got_rows = got_rows.reshape(sources, local, capacity, narrow)
    piece = lax.all_gather(got_rows, "tp", axis=3, tiled=True)
    gate = jnp.einsum("secd,edf->secf", piece, new_gate, preferred_element_type=jnp.float32)
    up = jnp.einsum("secd,edf->secf", piece, new_up, preferred_element_type=jnp.float32)
    factor = got_scale.reshape(sources, local, capacity)[..., None]
    weight = got_share.reshape(sources, local, capacity)[..., None]
    gate = gate * factor
    up = up * factor
    hidden_rows = (weight * jax.nn.silu(gate) * up).astype(jnp.bfloat16)
    hidden_rows = hidden_rows.reshape(sources * local, capacity, hidden_rows.shape[3])
    back = lax.all_to_all(hidden_rows, "fs", split_axis=0, concat_axis=0, tiled=True)
    picked = back.reshape(total, back.shape[2])[target].reshape(tok_rows, top, back.shape[2])
    return (new_gate, new_up, picked)


def dense_kernel(
    n, nt, width,
    tok_hbm, gain_hbm, gate_hbm, up_hbm, chosen_hbm, aff_hbm,
    served, hid_out,
    tok, wf, own, wsend, scale, hs, hr, gain, names_in, aff_in,
    ls_own_tok, ls_tok, ls_w, ls_own, ls_gain, ls_names, ls_aff,
    ss_tok, ss_w, ss_y, ss_h, rs_tz, rs_tx, rs_tm, rs_w, rs_y, rs_h, far,
):
    g, z, t = lax.axis_index("grp"), lax.axis_index("fs"), lax.axis_index("tp")
    depth, fcols = wf.shape[1], wf.shape[2]
    fc = fcols // CHUNKS
    mate = t + 1 - 2 * lax.rem(t, 2)
    xq = lax.rem(t + 2, nt)
    rows = tok.shape[1]
    has_up, has_dn = z + 1 < n, z > 0
    at_end = (z == 0) | (z == n - 1)

    def remote(src, dst, ssem, rsem, **dev):
        return pltpu.make_async_remote_copy(
            src_ref=src, dst_ref=dst, send_sem=ssem, recv_sem=rsem, device_id=dev, device_id_type=MESH
        )

    def local(src, dst, sem):
        return pltpu.make_async_copy(src, dst, sem)

    def signal(sem, **dev):
        pl.semaphore_signal(sem, 1, device_id=dev, device_id_type=MESH)

    barrier = pltpu.get_barrier_semaphore()
    for there, step in ((has_up, 1), (has_dn, -1)):

        @pl.when(there)
        def _():
            signal(barrier, fs=z + step)

    signal(barrier, grp=1 - g)
    signal(barrier, tp=mate)
    signal(barrier, tp=xq)

    def tok_load(q, sem):
        return local(
            tok_hbm.at[:, pl.ds(pl.multiple_of(q * depth, depth), depth)], tok.at[z * nt + q], sem
        )

    own_load = tok_load(t, ls_own_tok)
    own_load.start()
    small_loads = (
        local(gain_hbm, gain, ls_gain),
        local(chosen_hbm, names_in, ls_names),
        local(aff_hbm, aff_in, ls_aff),
    )
    small_loads[0].start()
    for off in range(1, n):
        e = lax.rem(z + off, n)

        @pl.when(g == 0)
        def _():
            local(gate_hbm.at[e], wf.at[off - 1], ls_w).start()

        @pl.when(g != 0)
        def _():
            local(up_hbm.at[e], wf.at[off - 1], ls_w).start()

    for m, ref in enumerate((gate_hbm, up_hbm)):
        local(ref.at[z], own.at[m], ls_own).start()
    for off in range(1, nt):
        tok_load(lax.rem(t + off, nt), ls_tok).start()
    for copy in small_loads[1:]:
        copy.start()

    half = rows // HALVES

    def block(s, q, h):
        return tok.at[s * nt + q, pl.ds(h * half, half)]

    def tz(s, step, h):
        ref = block(s, t, h)
        return remote(ref, ref, ss_tok, rs_tz.at[s, h], fs=z + step)

    def tx(s, h):
        ref = block(s, t, h)
        return remote(ref, ref, ss_tok, rs_tx.at[s, h], tp=xq)

    def tm(s, q, h):
        ref = block(s, q, h)
        return remote(ref, ref, ss_tok, rs_tm.at[s], tp=mate)

    def sides(d, fn):
        for sign in (1, -1):
            s = z + sign * d

            @pl.when((s >= 0) & (s < n))
            def _():
                fn(s, sign)

    own_load.wait()
    pl.semaphore_wait(barrier, 5 - jnp.where(at_end, 1, 0))

    for h in range(HALVES):
        sides(1, lambda s, sign: tz(z, sign, h).start())

    @pl.when(has_up & has_dn)
    def _():
        signal(far.at[0, 0], fs=z - 1)
        signal(far.at[1, 0], fs=z + 1)

    def slot(s):
        return lax.rem(s - z + n, n) - 1

    small_loads[0].wait()
    gcol = jnp.transpose(jnp.broadcast_to(gain[...], (128, depth)))
    gcol = jnp.concatenate([gcol] * (fc // 128), axis=1) if fc > 128 else gcol
    local(gate_hbm.at[pl.ds(0, n - 1)], wf, ls_w).wait()
    for k in range(n - 1):
        for c in range(CHUNKS):
            wsend[k, c] = (wf[k, :, c * fc : (c + 1) * fc] * gcol).astype(jnp.bfloat16)

    def hears(k, others, way, there, step):
        @pl.when(k < others)
        def _():
            pl.semaphore_wait(far.at[way, k], 1)
            if k + 1 < n - 2:

                @pl.when(there)
                def _():
                    signal(far.at[way, k + 1], fs=z + step)

    for k in range(n - 2):
        hears(k, n - 2 - z, 0, has_dn, -1)
        hears(k, z - 1, 1, has_up, 1)

    def part(s, p):
        size = depth // n
        return pl.ds(pl.multiple_of(s * depth + p * size, size), size)

    def strip(m, s, c, p):
        return served.at[m, part(s, p), pl.ds(c * fc, fc)]

    def wcopy(c, p, to):
        src = wsend.at[slot(to), c, part(0, p)]
        return remote(src, strip(g, z, c, p), ss_w, rs_w.at[c, p, z], fs=to)

    def send_weights(c, p, distances):
        for d in distances:
            sides(d, lambda s, sign: wcopy(c, p, s).start())

    @pl.when(at_end)
    def _():
        for c in range(CHUNKS):
            for p in range(n):
                send_weights(c, p, (1,))

    local(gate_hbm.at[pl.ds(0, 2)], own, ls_own).wait()
    for m in range(2):
        for c in range(CHUNKS):
            served[m, pl.ds(pl.multiple_of(z * depth, depth), depth), c * fc : (c + 1) * fc] = (
                own[m, :, c * fc : (c + 1) * fc] * gcol
            ).astype(jnp.bfloat16)

    def arrive_all(d):
        for h in range(HALVES):

            def arrive(s, sign):
                tz(s, 0, h).wait_recv()
                nxt = z - sign

                @pl.when((nxt >= 0) & (nxt < n))
                def _():
                    tz(s, -sign, h).start()

                tx(s, h).start()
                tm(s, t, h).start()

            sides(d, arrive)

    def xrelay(s, sign):
        for h in range(HALVES):
            tx(s, h).wait_recv()
            tm(s, xq, h).start()

    def ycopy(c, p, s):
        ref = strip(g, s, c, p)
        return remote(ref, ref, ss_y, rs_y.at[c], grp=1 - g)

    def yforward(c, p, d):
        def one(s, sign):
            ref = strip(g, s, c, p)
            remote(ref, ref, ss_w, rs_w.at[c, p, s], fs=s).wait_recv()
            ycopy(c, p, s).start()

        sides(d, one)

    def ywait(c):
        ref = wsend.at[:, c]
        remote(ref, ref, ss_y, rs_y.at[c], grp=1 - g).wait_recv()

    def hcopy(c, i, to):
        return remote(hs.at[i, c], hr.at[z, c], ss_h, rs_h.at[c], fs=to)

    def sumsq(s):
        part = jnp.zeros((rows, 128), jnp.float32)
        for q in range(nt):
            for i in range(depth // 128):
                x = tok[s * nt + q, :, i * 128 : (i + 1) * 128].astype(jnp.float32)
                part = part + x * x
        total = jnp.sum(part, axis=-1, keepdims=True)
        scale[s] = jnp.broadcast_to(lax.rsqrt(total / width + 1e-06), (rows, fc))

    def compute(c, i):
        rising = i + jnp.where(i >= z, 1, 0)
        falling = n - 1 - i - jnp.where(n - 1 - i <= z, 1, 0)
        s = jnp.where(i == n - 1, z, jnp.where(2 * z >= n, rising, falling))
        acc = None
        for q in range(nt):
            w = jnp.concatenate(
                [served[m, q * depth : (q + 1) * depth, c * fc : (c + 1) * fc] for m in range(2)], axis=1
            )
            term = jnp.dot(tok[s * nt + q], w, preferred_element_type=jnp.float32)
            acc = term if acc is None else acc + term
        gate = acc[:, :fc] * scale[s]
        up = acc[:, fc:] * scale[s]
        h = (gate / (1.0 + jnp.exp(-gate)) * up).astype(jnp.bfloat16)

        @pl.when(i < n - 1)
        def _():
            hs[i, c] = h
            hcopy(c, i, s).start()

        @pl.when(i == n - 1)
        def _():
            hr[z, c] = h

    arrive_all(1)
    for d in range(2, n - 1):
        arrive_all(d)

    @pl.when(at_end)
    def _():
        for c in range(CHUNKS):
            for p in range(n):
                send_weights(c, p, range(2, n))

    @pl.when(jnp.logical_not(at_end))
    def _():
        for c in range(CHUNKS):
            for p in range(n):
                send_weights(c, p, range(1, n))

    sides(1, xrelay)
    arrive_all(n - 1)
    for p in range(n):
        yforward(0, p, 1)
    for d in range(2, n):
        sides(d, xrelay)
        for p in range(n):
            yforward(0, p, d)

    local(tok_hbm.at[pl.ds(0, rows), pl.ds(0, (nt - 1) * depth)], tok_hbm.at[pl.ds(0, rows), pl.ds(0, (nt - 1) * depth)], ls_tok).wait()
    sumsq(z)

    def rest(s, sign):
        ref = tok.at[pl.ds(0, 2)]
        remote(ref, ref, ss_tok, rs_tm.at[s], tp=mate).wait_recv()
        sumsq(s)

    for d in range(1, n):
        sides(d, rest)
    ywait(0)

    def first(i, carry):
        for d in range(1, n):
            yforward(1, i, d)
        compute(0, i)
        return carry

    lax.fori_loop(0, n, first, 0)
    for copy in small_loads[1:]:
        copy.wait()
    aff = aff_in[...]
    share = aff / jnp.sum(aff, axis=0, keepdims=True)
    top = aff.shape[0]

    def column(row):
        col = jnp.transpose(jnp.broadcast_to(row, (128, rows)))
        return jnp.concatenate([col] * (fc // 128), axis=1) if fc > 128 else col

    shares = [column(share[k : k + 1, :]) for k in range(top)]
    names = [column(names_in[k : k + 1, :].astype(jnp.float32)) for k in range(top)]
    ywait(1)

    def second(i, carry):
        compute(1, i)
        return carry

    lax.fori_loop(0, n, second, 0)

    for c in range(CHUNKS):
        ref = hs.at[:, c]
        remote(ref, ref, ss_h, rs_h.at[c], fs=z).wait_recv()
        picks = []
        for k in range(top):
            picked = jnp.zeros((rows, fc), jnp.float32)
            for e in range(n):
                picked = jnp.where(names[k] == e, hr[e, c].astype(jnp.float32), picked)
            picks.append(picked * shares[k])
        hid_out[:, :, c * fc : (c + 1) * fc] = jnp.stack(picks, axis=1).astype(jnp.bfloat16)

    def sent(ref, sem):
        remote(ref, ref, sem, rs_h.at[0], fs=z).wait_send()

    relayed = 3 * (n - 1)

    @pl.when(at_end)
    def _():
        sent(tok.at[pl.ds(0, relayed + 1)], ss_tok)

    @pl.when(jnp.logical_not(at_end))
    def _():
        sent(tok.at[pl.ds(0, relayed + n + 1)], ss_tok)

    sent(wsend, ss_w)
    sent(wsend, ss_y)
    sent(hs, ss_h)


def emit_kernel(served, hid, gate_out, up_out, hid_out, sems):
    copies = [
        pltpu.make_async_copy(hid, hid_out, sems.at[2]),
        pltpu.make_async_copy(served.at[0], gate_out.at[0], sems.at[0]),
        pltpu.make_async_copy(served.at[1], up_out.at[0], sems.at[1]),
    ]
    for copy in copies:
        copy.start()
    for copy in copies:
        copy.wait()


def dense(tokens, norm_gain, gate_master, up_master, chosen, affinity):
    n, nt = lax.axis_size("fs"), lax.axis_size("tp")
    rows, width = tokens.shape
    experts, depth, fcols = gate_master.shape
    top = chosen.shape[1]
    fc = fcols // CHUNKS
    bf, f32 = jnp.bfloat16, jnp.float32
    dma = pltpu.SemaphoreType.DMA
    hbm = pl.BlockSpec(memory_space=pltpu.HBM)
    vmem = pl.BlockSpec(memory_space=pltpu.VMEM)
    served, hid = pl.pallas_call(
        functools.partial(dense_kernel, n, nt, width),
        out_shape=(
            jax.ShapeDtypeStruct((2, width, fcols), bf),
            jax.ShapeDtypeStruct((rows, top, fcols), bf),
        ),
        in_specs=[hbm] * 6,
        out_specs=(vmem, vmem),
        scratch_shapes=[
            pltpu.VMEM((n * nt, rows, depth), bf),
            pltpu.VMEM((n - 1, depth, fcols), f32),
            pltpu.VMEM((2, depth, fcols), f32),
            pltpu.VMEM((n - 1, CHUNKS, depth, fc), bf),
            pltpu.VMEM((n, rows, fc), f32),
            pltpu.VMEM((n - 1, CHUNKS, rows, fc), bf),
            pltpu.VMEM((n, CHUNKS, rows, fc), bf),
            pltpu.VMEM((1, depth), f32),
            pltpu.VMEM((top, rows), jnp.int32),
            pltpu.VMEM((top, rows), f32),
            dma, dma, dma, dma, dma, dma, dma,
            dma, dma, dma, dma,
            dma((n, HALVES)),
            dma((n, HALVES)),
            dma((n,)),
            dma((CHUNKS, n, n)),
            dma((CHUNKS,)),
            dma((CHUNKS,)),
            pltpu.SemaphoreType.REGULAR((2, n - 2)),
        ],
        compiler_params=pltpu.CompilerParams(
            collective_id=0, has_side_effects=True, vmem_limit_bytes=40 * 1024 * 1024
        ),
    )(*[pltpu.with_memory_space_constraint(x, pltpu.HBM) for x in (tokens, norm_gain.reshape(1, depth), gate_master, up_master, chosen.T, affinity.T)])
    return pl.pallas_call(
        emit_kernel,
        out_shape=(
            jax.ShapeDtypeStruct((1, width, fcols), bf),
            jax.ShapeDtypeStruct((1, width, fcols), bf),
            jax.ShapeDtypeStruct((rows, top, fcols), bf),
        ),
        in_specs=[vmem, vmem],
        out_specs=(hbm, hbm, hbm),
        scratch_shapes=[dma((3,))],
        compiler_params=pltpu.CompilerParams(vmem_limit_bytes=1024 * 1024),
    )(served, hid)


def on_device(tokens, norm_gain, gate_master, up_master, chosen, affinity):
    n, nt = lax.axis_size("fs"), lax.axis_size("tp")
    experts, depth, fcols = gate_master.shape
    rows, width = tokens.shape
    capacity = rows * chosen.shape[1] * 2 // experts
    fits = (
        experts == n
        and capacity >= rows
        and n >= 3
        and nt == 4
        and lax.axis_size("grp") == 2
        and width == nt * depth
        and fcols % (CHUNKS * 128) == 0
        and depth % (16 * n) == 0
    )
    run = dense if fits else routed
    return run(tokens, norm_gain, gate_master, up_master, chosen, affinity)


def solution(mesh):
    return jax.shard_map(
        on_device,
        mesh=mesh,
        in_specs=(
            P(("grp", "fs"), None),
            P("fs"),
            P(None, "fs", "tp"),
            P(None, "fs", "tp"),
            P(("grp", "fs"), None),
            P(("grp", "fs"), None),
        ),
        out_specs=(
            P(("grp", "fs"), None, "tp"),
            P(("grp", "fs"), None, "tp"),
            P(("grp", "fs"), None, "tp"),
        ),
        check_vma=False,
    )
```

```python
import functools

import jax
import jax.numpy as jnp
from jax import lax
from jax.experimental import pallas as pl
from jax.experimental.pallas import tpu as pltpu
from jax.sharding import PartitionSpec as P

MESH = pl.DeviceIdType.MESH
CHUNKS = 2
HALVES = 2


def routed(tokens, norm_gain, gate_master, up_master, chosen, affinity):
    folded_gate = (gate_master * norm_gain[None, :, None]).astype(jnp.bfloat16)
    folded_up = (up_master * norm_gain[None, :, None]).astype(jnp.bfloat16)
    new_gate, new_up = (
        lax.all_to_all(folded_gate, "fs", split_axis=0, concat_axis=1, tiled=True),
        lax.all_to_all(folded_up, "fs", split_axis=0, concat_axis=1, tiled=True),
    )
    experts_all = gate_master.shape[0]
    tok_rows, width = tokens.shape
    top = chosen.shape[1]
    capacity = tok_rows * top * 2 // experts_all
    local = new_gate.shape[0]
    xfloat = tokens.astype(jnp.float32)
    scale = lax.rsqrt(jnp.mean(xfloat * xfloat, axis=-1) + 1e-06)
    share = affinity / jnp.sum(affinity, axis=-1, keepdims=True)
    flat_e = chosen.reshape(-1)
    onehot = (flat_e[:, None] == jnp.arange(experts_all, dtype=jnp.int32)[None, :]).astype(
        jnp.int32
    )
    slot = jnp.sum((jnp.cumsum(onehot, axis=0) - onehot) * onehot, axis=1)
    target = flat_e * capacity + slot
    owner = jnp.repeat(jnp.arange(tok_rows, dtype=jnp.int32), top)
    total = experts_all * capacity
    scale_buf = (
        jnp.zeros((total,), jnp.float32).at[target].set(scale[owner]).reshape(experts_all, capacity)
    )
    share_buf = (
        jnp.zeros((total,), jnp.float32)
        .at[target]
        .set(share.reshape(-1))
        .reshape(experts_all, capacity)
    )
    narrow = width // lax.axis_size("tp")
    own_cols = lax.dynamic_slice_in_dim(tokens, lax.axis_index("tp") * narrow, narrow, 1)
    row_buf = jnp.zeros((total, narrow), jnp.bfloat16).at[target].set(own_cols[owner])
    row_buf = row_buf.reshape(experts_all, capacity, narrow)
    got_rows, got_scale, got_share = (
        lax.all_to_all(row_buf, "fs", split_axis=0, concat_axis=0, tiled=True),
        lax.all_to_all(
            scale_buf.astype(jnp.bfloat16), "fs", split_axis=0, concat_axis=0, tiled=True
        ).astype(scale_buf.dtype),
        lax.all_to_all(
            share_buf.astype(jnp.bfloat16), "fs", split_axis=0, concat_axis=0, tiled=True
        ).astype(share_buf.dtype),
    )
    sources = got_rows.shape[0] // local
    got_rows = got_rows.reshape(sources, local, capacity, narrow)
    piece = lax.all_gather(got_rows, "tp", axis=3, tiled=True)
    gate = jnp.einsum("secd,edf->secf", piece, new_gate, preferred_element_type=jnp.float32)
    up = jnp.einsum("secd,edf->secf", piece, new_up, preferred_element_type=jnp.float32)
    factor = got_scale.reshape(sources, local, capacity)[..., None]
    weight = got_share.reshape(sources, local, capacity)[..., None]
    gate = gate * factor
    up = up * factor
    hidden_rows = (weight * jax.nn.silu(gate) * up).astype(jnp.bfloat16)
    hidden_rows = hidden_rows.reshape(sources * local, capacity, hidden_rows.shape[3])
    back = lax.all_to_all(hidden_rows, "fs", split_axis=0, concat_axis=0, tiled=True)
    picked = back.reshape(total, back.shape[2])[target].reshape(tok_rows, top, back.shape[2])
    return (new_gate, new_up, picked)


def dense_kernel(
    n, nt, width,
    tok_hbm, gain_hbm, gate_hbm, up_hbm, chosen_hbm, aff_hbm,
    served, hid_out,
    tok, wf, own, wsend, scale, hs, hr, gain, names_in, aff_in,
    ls_own_tok, ls_tok, ls_w, ls_own, ls_gain, ls_names, ls_aff,
    ss_tok, ss_w, ss_y, ss_h, rs_tz, rs_tx, rs_tm, rs_w, rs_y, rs_h, far,
):
    g, z, t = lax.axis_index("grp"), lax.axis_index("fs"), lax.axis_index("tp")
    depth, fcols = wf.shape[1], wf.shape[2]
    fc = fcols // CHUNKS
    mate = t + 1 - 2 * lax.rem(t, 2)
    xq = lax.rem(t + 2, nt)
    rows = tok.shape[1]
    has_up, has_dn = z + 1 < n, z > 0
    at_end = (z == 0) | (z == n - 1)

    def remote(src, dst, ssem, rsem, **dev):
        return pltpu.make_async_remote_copy(
            src_ref=src, dst_ref=dst, send_sem=ssem, recv_sem=rsem, device_id=dev, device_id_type=MESH
        )

    def local(src, dst, sem):
        return pltpu.make_async_copy(src, dst, sem)

    def signal(sem, **dev):
        pl.semaphore_signal(sem, 1, device_id=dev, device_id_type=MESH)

    barrier = pltpu.get_barrier_semaphore()
    for there, step in ((has_up, 1), (has_dn, -1)):

        @pl.when(there)
        def _():
            signal(barrier, fs=z + step)

    signal(barrier, grp=1 - g)
    signal(barrier, tp=mate)
    signal(barrier, tp=xq)

    def tok_load(q, sem):
        return local(
            tok_hbm.at[:, pl.ds(pl.multiple_of(q * depth, depth), depth)], tok.at[z * nt + q], sem
        )

    own_load = tok_load(t, ls_own_tok)
    own_load.start()
    small_loads = (
        local(gain_hbm, gain, ls_gain),
        local(chosen_hbm, names_in, ls_names),
        local(aff_hbm, aff_in, ls_aff),
    )
    small_loads[0].start()
    for off in range(1, n):
        e = lax.rem(z + off, n)

        @pl.when(g == 0)
        def _():
            local(gate_hbm.at[e], wf.at[off - 1], ls_w).start()

        @pl.when(g != 0)
        def _():
            local(up_hbm.at[e], wf.at[off - 1], ls_w).start()

    for m, ref in enumerate((gate_hbm, up_hbm)):
        local(ref.at[z], own.at[m], ls_own).start()
    for off in range(1, nt):
        tok_load(lax.rem(t + off, nt), ls_tok).start()
    for copy in small_loads[1:]:
        copy.start()

    half = rows // HALVES

    def block(s, q, h):
        return tok.at[s * nt + q, pl.ds(h * half, half)]

    def tz(s, step, h):
        ref = block(s, t, h)
        return remote(ref, ref, ss_tok, rs_tz.at[s, h], fs=z + step)

    def tx(s, h):
        ref = block(s, t, h)
        return remote(ref, ref, ss_tok, rs_tx.at[s, h], tp=xq)

    def tm(s, q, h):
        ref = block(s, q, h)
        return remote(ref, ref, ss_tok, rs_tm.at[s], tp=mate)

    def sides(d, fn):
        for sign in (1, -1):
            s = z + sign * d

            @pl.when((s >= 0) & (s < n))
            def _():
                fn(s, sign)

    with jax.named_scope('barrier'):
        own_load.wait()
        pl.semaphore_wait(barrier, 5 - jnp.where(at_end, 1, 0))

    for h in range(HALVES):
        sides(1, lambda s, sign: tz(z, sign, h).start())

    @pl.when(has_up & has_dn)
    def _():
        signal(far.at[0, 0], fs=z - 1)
        signal(far.at[1, 0], fs=z + 1)

    def slot(s):
        return lax.rem(s - z + n, n) - 1

    with jax.named_scope('gain'):
        small_loads[0].wait()
    gcol = jnp.transpose(jnp.broadcast_to(gain[...], (128, depth)))
    gcol = jnp.concatenate([gcol] * (fc // 128), axis=1) if fc > 128 else gcol
    with jax.named_scope('wload'):
        local(gate_hbm.at[pl.ds(0, n - 1)], wf, ls_w).wait()
    for k in range(n - 1):
        for c in range(CHUNKS):
            wsend[k, c] = (wf[k, :, c * fc : (c + 1) * fc] * gcol).astype(jnp.bfloat16)

    def hears(k, others, way, there, step):
        @pl.when(k < others)
        def _():
            pl.semaphore_wait(far.at[way, k], 1)
            if k + 1 < n - 2:

                @pl.when(there)
                def _():
                    signal(far.at[way, k + 1], fs=z + step)

    def part(s, p):
        size = depth // n
        return pl.ds(pl.multiple_of(s * depth + p * size, size), size)

    def strip(m, s, c, p):
        return served.at[m, part(s, p), pl.ds(c * fc, fc)]

    def wcopy(c, p, to):
        src = wsend.at[slot(to), c, part(0, p)]
        return remote(src, strip(g, z, c, p), ss_w, rs_w.at[c, p, z], fs=to)

    def send_weights(c, d, sign):
        for p in range(n):
            wcopy(c, p, z + sign * d).start()

    for c in range(CHUNKS):
        for there, sign in ((has_up, 1), (has_dn, -1)):
            pl.when(there)(functools.partial(send_weights, c, 1, sign))

    with jax.named_scope('hears'):
        for k in range(n - 2):
            hears(k, n - 2 - z, 0, has_dn, -1)
            hears(k, z - 1, 1, has_up, 1)

    local(gate_hbm.at[pl.ds(0, 2)], own, ls_own).wait()
    for m in range(2):
        for c in range(CHUNKS):
            served[m, pl.ds(pl.multiple_of(z * depth, depth), depth), c * fc : (c + 1) * fc] = (
                own[m, :, c * fc : (c + 1) * fc] * gcol
            ).astype(jnp.bfloat16)

    def arrive_all(d):
        for h in range(HALVES):

            def arrive(s, sign):
                tz(s, 0, h).wait_recv()
                nxt = z - sign

                @pl.when((nxt >= 0) & (nxt < n))
                def _():
                    tz(s, -sign, h).start()

                tx(s, h).start()
                tm(s, t, h).start()

            sides(d, arrive)

    def xrelay(s, sign):
        for h in range(HALVES):
            tx(s, h).wait_recv()
            tm(s, xq, h).start()

    def ycopy(c, p, s):
        ref = strip(g, s, c, p)
        return remote(ref, ref, ss_y, rs_y.at[c], grp=1 - g)

    def yforward(c, d, side=None):
        def one(s, sign):
            for p in range(n):
                ref = strip(g, s, c, p)
                remote(ref, ref, ss_w, rs_w.at[c, p, s], fs=s).wait_recv()
                ycopy(c, p, s).start()

        def one_side(s, sign):
            outer = (s == 0) | (s == n - 1)
            pl.when(outer if side == "outer" else jnp.logical_not(outer))(lambda: one(s, sign))

        sides(d, one_side if side else one)

    def ywait(c):
        ref = wsend.at[:, c]
        remote(ref, ref, ss_y, rs_y.at[c], grp=1 - g).wait_recv()

    def hcopy(c, i, to):
        return remote(hs.at[i, c], hr.at[z, c], ss_h, rs_h.at[c], fs=to)

    def sumsq(s):
        part = jnp.zeros((rows, 128), jnp.float32)
        for q in range(nt):
            for i in range(depth // 128):
                x = tok[s * nt + q, :, i * 128 : (i + 1) * 128].astype(jnp.float32)
                part = part + x * x
        total = jnp.sum(part, axis=-1, keepdims=True)
        scale[s] = jnp.broadcast_to(lax.rsqrt(total / width + 1e-06), (rows, fc))

    def compute(c, i):
        rising = i + jnp.where(i >= z, 1, 0)
        falling = n - 1 - i - jnp.where(n - 1 - i <= z, 1, 0)
        s = jnp.where(i == n - 1, z, jnp.where(2 * z >= n, rising, falling))
        strips = pl.ds(pl.multiple_of(c * fc, fc), fc)
        acc = None
        for q in range(nt):
            w = jnp.concatenate(
                [served[m, q * depth : (q + 1) * depth, strips] for m in range(2)], axis=1
            )
            term = jnp.dot(tok[s * nt + q], w, preferred_element_type=jnp.float32)
            acc = term if acc is None else acc + term
        gate = acc[:, :fc] * scale[s]
        up = acc[:, fc:] * scale[s]
        h = (gate / (1.0 + jnp.exp(-gate)) * up).astype(jnp.bfloat16)

        @pl.when(i < n - 1)
        def _():
            hs[i, c] = h
            hcopy(c, i, s).start()

        @pl.when(i == n - 1)
        def _():
            hr[z, c] = h

    inner = jnp.logical_not(at_end)
    late = lax.rem(t, 2) == 1

    def send_far():
        for d in range(2, n):
            for c in range(CHUNKS):
                for sign in (1, -1):
                    s = z + sign * d
                    pl.when((s >= 0) & (s < n))(functools.partial(send_weights, c, d, sign))

    with jax.named_scope("arr1"):
        arrive_all(1)

    local(
        tok_hbm.at[:, pl.ds(0, (nt - 1) * depth)], tok_hbm.at[:, pl.ds(0, (nt - 1) * depth)], ls_tok
    ).wait()
    sumsq(z)

    def rest(s, sign):
        ref = tok.at[pl.ds(0, 2)]
        remote(ref, ref, ss_tok, rs_tm.at[s], tp=mate).wait_recv()
        sumsq(s)

    def totals():
        with jax.named_scope("rest"):
            for d in range(1, n):
                sides(d, rest)

    @pl.when(at_end)
    def _():
        with jax.named_scope("yf0_1"):
            yforward(0, 1)
        with jax.named_scope("xr1"):
            sides(1, xrelay)
        with jax.named_scope("yf1_1"):
            yforward(1, 1)
        for d in range(2, n - 1):
            with jax.named_scope("arr2"):
                arrive_all(d)
        send_far()
        for d in range(2, n - 1):
            with jax.named_scope("xr2"):
                sides(d, xrelay)
        with jax.named_scope("arr3"):
            arrive_all(n - 1)
        with jax.named_scope("yf0_3"):
            yforward(0, n - 1)
        with jax.named_scope("xr3"):
            sides(n - 1, xrelay)
        with jax.named_scope("yf1_3"):
            yforward(1, n - 1)
        totals()
        for c in range(CHUNKS):
            for d in range(2, n - 1):
                with jax.named_scope("yf%d_2" % c):
                    yforward(c, d)

    @pl.when(inner)
    def _():
        for c in range(CHUNKS):
            with jax.named_scope("yf%d_1" % c):
                yforward(c, 1)
        with jax.named_scope("xr1"):
            sides(1, xrelay)
        for d in range(2, n - 1):
            with jax.named_scope("arr2"):
                arrive_all(d)
        for d in range(2, n - 1):
            with jax.named_scope("yf0_2"):
                yforward(0, d)
        send_far()
        for d in range(2, n - 1):
            with jax.named_scope("xr2"):
                sides(d, xrelay)
        for d in range(2, n - 1):
            with jax.named_scope("yf1_2"):
                yforward(1, d)
        totals()

    for copy in small_loads[1:]:
        copy.wait()
    aff = aff_in[...]
    share = aff / jnp.sum(aff, axis=0, keepdims=True)
    top = aff.shape[0]

    def column(row):
        col = jnp.transpose(jnp.broadcast_to(row, (128, rows)))
        return jnp.concatenate([col] * (fc // 128), axis=1) if fc > 128 else col

    shares = [column(share[k : k + 1, :]) for k in range(top)]
    names = [column(names_in[k : k + 1, :].astype(jnp.float32)) for k in range(top)]
    with jax.named_scope("yw0"):
        ywait(0)

    def step(j, carry):
        @pl.when(j == jnp.where(at_end, n, 0))
        def _():
            with jax.named_scope("yw1"):
                ywait(1)

        c = jnp.where(at_end, j // n, lax.rem(j, CHUNKS))
        i = jnp.where(at_end, lax.rem(j, n), j // CHUNKS)
        with jax.named_scope("comp"):
            compute(c, i)
        return carry

    lax.fori_loop(0, n * CHUNKS, step, 0)

    for c in range(CHUNKS):
        ref = hs.at[:, c]
        with jax.named_scope('hw%d' % c):
            remote(ref, ref, ss_h, rs_h.at[c], fs=z).wait_recv()
        picks = []
        for k in range(top):
            picked = jnp.zeros((rows, fc), jnp.float32)
            for e in range(n):
                picked = jnp.where(names[k] == e, hr[e, c].astype(jnp.float32), picked)
            picks.append(picked * shares[k])
        hid_out[:, :, c * fc : (c + 1) * fc] = jnp.stack(picks, axis=1).astype(jnp.bfloat16)

    def sent(ref, sem):
      with jax.named_scope('sent'):
        remote(ref, ref, sem, rs_h.at[0], fs=z).wait_send()

    relayed = 3 * (n - 1)

    @pl.when(at_end)
    def _():
        sent(tok.at[pl.ds(0, relayed + 1)], ss_tok)

    @pl.when(jnp.logical_not(at_end))
    def _():
        sent(tok.at[pl.ds(0, relayed + n + 1)], ss_tok)

    sent(wsend, ss_w)
    sent(wsend, ss_y)
    sent(hs, ss_h)


def emit_kernel(served, hid, gate_out, up_out, hid_out, sems):
    copies = [
        pltpu.make_async_copy(hid, hid_out, sems.at[2]),
        pltpu.make_async_copy(served.at[0], gate_out.at[0], sems.at[0]),
        pltpu.make_async_copy(served.at[1], up_out.at[0], sems.at[1]),
    ]
    for copy in copies:
        copy.start()
    for copy in copies:
        copy.wait()


def dense(tokens, norm_gain, gate_master, up_master, chosen, affinity):
    n, nt = lax.axis_size("fs"), lax.axis_size("tp")
    rows, width = tokens.shape
    experts, depth, fcols = gate_master.shape
    top = chosen.shape[1]
    fc = fcols // CHUNKS
    bf, f32 = jnp.bfloat16, jnp.float32
    dma = pltpu.SemaphoreType.DMA
    hbm = pl.BlockSpec(memory_space=pltpu.HBM)
    vmem = pl.BlockSpec(memory_space=pltpu.VMEM)
    served, hid = pl.pallas_call(
        functools.partial(dense_kernel, n, nt, width),
        out_shape=(
            jax.ShapeDtypeStruct((2, width, fcols), bf),
            jax.ShapeDtypeStruct((rows, top, fcols), bf),
        ),
        in_specs=[hbm] * 6,
        out_specs=(vmem, vmem),
        scratch_shapes=[
            pltpu.VMEM((n * nt, rows, depth), bf),
            pltpu.VMEM((n - 1, depth, fcols), f32),
            pltpu.VMEM((2, depth, fcols), f32),
            pltpu.VMEM((n - 1, CHUNKS, depth, fc), bf),
            pltpu.VMEM((n, rows, fc), f32),
            pltpu.VMEM((n - 1, CHUNKS, rows, fc), bf),
            pltpu.VMEM((n, CHUNKS, rows, fc), bf),
            pltpu.VMEM((1, depth), f32),
            pltpu.VMEM((top, rows), jnp.int32),
            pltpu.VMEM((top, rows), f32),
            dma, dma, dma, dma, dma, dma, dma,
            dma, dma, dma, dma,
            dma((n, HALVES)),
            dma((n, HALVES)),
            dma((n,)),
            dma((CHUNKS, n, n)),
            dma((CHUNKS,)),
            dma((CHUNKS,)),
            pltpu.SemaphoreType.REGULAR((2, n - 2)),
        ],
        compiler_params=pltpu.CompilerParams(
            collective_id=0, has_side_effects=True, vmem_limit_bytes=40 * 1024 * 1024
        ),
    )(*[pltpu.with_memory_space_constraint(x, pltpu.HBM) for x in (tokens, norm_gain.reshape(1, depth), gate_master, up_master, chosen.T, affinity.T)])
    return pl.pallas_call(
        emit_kernel,
        out_shape=(
            jax.ShapeDtypeStruct((1, width, fcols), bf),
            jax.ShapeDtypeStruct((1, width, fcols), bf),
            jax.ShapeDtypeStruct((rows, top, fcols), bf),
        ),
        in_specs=[vmem, vmem],
        out_specs=(hbm, hbm, hbm),
        scratch_shapes=[dma((3,))],
        compiler_params=pltpu.CompilerParams(vmem_limit_bytes=1024 * 1024),
    )(served, hid)


def on_device(tokens, norm_gain, gate_master, up_master, chosen, affinity):
    n, nt = lax.axis_size("fs"), lax.axis_size("tp")
    experts, depth, fcols = gate_master.shape
    rows, width = tokens.shape
    capacity = rows * chosen.shape[1] * 2 // experts
    fits = (
        experts == n
        and capacity >= rows
        and n >= 3
        and nt == 4
        and lax.axis_size("grp") == 2
        and width == nt * depth
        and fcols % (CHUNKS * 128) == 0
        and depth % (16 * n) == 0
    )
    run = dense if fits else routed
    return run(tokens, norm_gain, gate_master, up_master, chosen, affinity)


def solution(mesh):
    return jax.shard_map(
        on_device,
        mesh=mesh,
        in_specs=(
            P(("grp", "fs"), None),
            P("fs"),
            P(None, "fs", "tp"),
            P(None, "fs", "tp"),
            P(("grp", "fs"), None),
            P(("grp", "fs"), None),
        ),
        out_specs=(
            P(("grp", "fs"), None, "tp"),
            P(("grp", "fs"), None, "tp"),
            P(("grp", "fs"), None, "tp"),
        ),
        check_vma=False,
    )
```

```python
import functools

import jax
import jax.numpy as jnp
from jax import lax
from jax.experimental import pallas as pl
from jax.experimental.pallas import tpu as pltpu
from jax.sharding import PartitionSpec as P

MESH = pl.DeviceIdType.MESH
CHUNKS = 2
HALVES = 2


def routed(tokens, norm_gain, gate_master, up_master, chosen, affinity):
    folded_gate = (gate_master * norm_gain[None, :, None]).astype(jnp.bfloat16)
    folded_up = (up_master * norm_gain[None, :, None]).astype(jnp.bfloat16)
    new_gate, new_up = (
        lax.all_to_all(folded_gate, "fs", split_axis=0, concat_axis=1, tiled=True),
        lax.all_to_all(folded_up, "fs", split_axis=0, concat_axis=1, tiled=True),
    )
    experts_all = gate_master.shape[0]
    tok_rows, width = tokens.shape
    top = chosen.shape[1]
    capacity = tok_rows * top * 2 // experts_all
    local = new_gate.shape[0]
    xfloat = tokens.astype(jnp.float32)
    scale = lax.rsqrt(jnp.mean(xfloat * xfloat, axis=-1) + 1e-06)
    share = affinity / jnp.sum(affinity, axis=-1, keepdims=True)
    flat_e = chosen.reshape(-1)
    onehot = (flat_e[:, None] == jnp.arange(experts_all, dtype=jnp.int32)[None, :]).astype(
        jnp.int32
    )
    slot = jnp.sum((jnp.cumsum(onehot, axis=0) - onehot) * onehot, axis=1)
    target = flat_e * capacity + slot
    owner = jnp.repeat(jnp.arange(tok_rows, dtype=jnp.int32), top)
    total = experts_all * capacity
    scale_buf = (
        jnp.zeros((total,), jnp.float32).at[target].set(scale[owner]).reshape(experts_all, capacity)
    )
    share_buf = (
        jnp.zeros((total,), jnp.float32)
        .at[target]
        .set(share.reshape(-1))
        .reshape(experts_all, capacity)
    )
    narrow = width // lax.axis_size("tp")
    own_cols = lax.dynamic_slice_in_dim(tokens, lax.axis_index("tp") * narrow, narrow, 1)
    row_buf = jnp.zeros((total, narrow), jnp.bfloat16).at[target].set(own_cols[owner])
    row_buf = row_buf.reshape(experts_all, capacity, narrow)
    got_rows, got_scale, got_share = (
        lax.all_to_all(row_buf, "fs", split_axis=0, concat_axis=0, tiled=True),
        lax.all_to_all(
            scale_buf.astype(jnp.bfloat16), "fs", split_axis=0, concat_axis=0, tiled=True
        ).astype(scale_buf.dtype),
        lax.all_to_all(
            share_buf.astype(jnp.bfloat16), "fs", split_axis=0, concat_axis=0, tiled=True
        ).astype(share_buf.dtype),
    )
    sources = got_rows.shape[0] // local
    got_rows = got_rows.reshape(sources, local, capacity, narrow)
    piece = lax.all_gather(got_rows, "tp", axis=3, tiled=True)
    gate = jnp.einsum("secd,edf->secf", piece, new_gate, preferred_element_type=jnp.float32)
    up = jnp.einsum("secd,edf->secf", piece, new_up, preferred_element_type=jnp.float32)
    factor = got_scale.reshape(sources, local, capacity)[..., None]
    weight = got_share.reshape(sources, local, capacity)[..., None]
    gate = gate * factor
    up = up * factor
    hidden_rows = (weight * jax.nn.silu(gate) * up).astype(jnp.bfloat16)
    hidden_rows = hidden_rows.reshape(sources * local, capacity, hidden_rows.shape[3])
    back = lax.all_to_all(hidden_rows, "fs", split_axis=0, concat_axis=0, tiled=True)
    picked = back.reshape(total, back.shape[2])[target].reshape(tok_rows, top, back.shape[2])
    return (new_gate, new_up, picked)


def dense_kernel(
    n, nt, width,
    tok_hbm, gain_hbm, gate_hbm, up_hbm, chosen_hbm, aff_hbm,
    served, hid_out,
    tok, wf, own, wsend, scale, hs, hr, gain, names_in, aff_in,
    ls_own_tok, ls_tok, ls_w, ls_own, ls_gain, ls_names, ls_aff,
    ss_tok, ss_w, ss_y, ss_h, rs_tz, rs_tx, rs_tm, rs_w, rs_y, rs_h, far,
):
    g, z, t = lax.axis_index("grp"), lax.axis_index("fs"), lax.axis_index("tp")
    depth, fcols = wf.shape[1], wf.shape[2]
    fc = fcols // CHUNKS
    mate = t + 1 - 2 * lax.rem(t, 2)
    xq = lax.rem(t + 2, nt)
    rows = tok.shape[1]
    has_up, has_dn = z + 1 < n, z > 0
    at_end = (z == 0) | (z == n - 1)

    def remote(src, dst, ssem, rsem, **dev):
        return pltpu.make_async_remote_copy(
            src_ref=src, dst_ref=dst, send_sem=ssem, recv_sem=rsem, device_id=dev, device_id_type=MESH
        )

    def local(src, dst, sem):
        return pltpu.make_async_copy(src, dst, sem)

    def signal(sem, **dev):
        pl.semaphore_signal(sem, 1, device_id=dev, device_id_type=MESH)

    barrier = pltpu.get_barrier_semaphore()
    for there, step in ((has_up, 1), (has_dn, -1)):

        @pl.when(there)
        def _():
            signal(barrier, fs=z + step)

    signal(barrier, grp=1 - g)
    signal(barrier, tp=mate)
    signal(barrier, tp=xq)

    def tok_load(q, sem):
        return local(
            tok_hbm.at[:, pl.ds(pl.multiple_of(q * depth, depth), depth)], tok.at[z * nt + q], sem
        )

    own_load = tok_load(t, ls_own_tok)
    own_load.start()
    small_loads = (
        local(gain_hbm, gain, ls_gain),
        local(chosen_hbm, names_in, ls_names),
        local(aff_hbm, aff_in, ls_aff),
    )
    small_loads[0].start()
    for off in range(1, n):
        e = lax.rem(z + off, n)

        @pl.when(g == 0)
        def _():
            local(gate_hbm.at[e], wf.at[off - 1], ls_w).start()

        @pl.when(g != 0)
        def _():
            local(up_hbm.at[e], wf.at[off - 1], ls_w).start()

    for m, ref in enumerate((gate_hbm, up_hbm)):
        local(ref.at[z], own.at[m], ls_own).start()
    for off in range(1, nt):
        tok_load(lax.rem(t + off, nt), ls_tok).start()
    for copy in small_loads[1:]:
        copy.start()

    half = rows // HALVES

    def block(s, q, h):
        return tok.at[s * nt + q, pl.ds(h * half, half)]

    def tz(s, step, h):
        ref = block(s, t, h)
        return remote(ref, ref, ss_tok, rs_tz.at[s, h], fs=z + step)

    def tx(s, h):
        ref = block(s, t, h)
        return remote(ref, ref, ss_tok, rs_tx.at[s, h], tp=xq)

    def tm(s, q, h):
        ref = block(s, q, h)
        return remote(ref, ref, ss_tok, rs_tm.at[s], tp=mate)

    def sides(d, fn):
        for sign in (1, -1):
            s = z + sign * d

            @pl.when((s >= 0) & (s < n))
            def _():
                fn(s, sign)

    with jax.named_scope('barrier'):
        own_load.wait()
        pl.semaphore_wait(barrier, 5 - jnp.where(at_end, 1, 0))

    for h in range(HALVES):
        sides(1, lambda s, sign: tz(z, sign, h).start())

    @pl.when(has_up & has_dn)
    def _():
        signal(far.at[0, 0], fs=z - 1)
        signal(far.at[1, 0], fs=z + 1)

    def slot(s):
        return lax.rem(s - z + n, n) - 1

    with jax.named_scope('gain'):
        small_loads[0].wait()
    gcol = jnp.transpose(jnp.broadcast_to(gain[...], (128, depth)))
    gcol = jnp.concatenate([gcol] * (fc // 128), axis=1) if fc > 128 else gcol
    with jax.named_scope('wload'):
        local(gate_hbm.at[pl.ds(0, n - 1)], wf, ls_w).wait()
    for k in range(n - 1):
        for c in range(CHUNKS):
            wsend[k, c] = (wf[k, :, c * fc : (c + 1) * fc] * gcol).astype(jnp.bfloat16)

    def hears(k, others, way, there, step):
        @pl.when(k < others)
        def _():
            pl.semaphore_wait(far.at[way, k], 1)
            if k + 1 < n - 2:

                @pl.when(there)
                def _():
                    signal(far.at[way, k + 1], fs=z + step)

    def part(s, p):
        size = depth // n
        return pl.ds(pl.multiple_of(s * depth + p * size, size), size)

    def strip(m, s, c, p):
        return served.at[m, part(s, p), pl.ds(c * fc, fc)]

    def wcopy(c, p, to):
        src = wsend.at[slot(to), c, part(0, p)]
        return remote(src, strip(g, z, c, p), ss_w, rs_w.at[c, p, z], fs=to)

    def send_weights(c, d, sign):
        for p in range(n):
            wcopy(c, p, z + sign * d).start()

    for c in range(CHUNKS):
        for there, sign in ((has_up, 1), (has_dn, -1)):
            pl.when(there)(functools.partial(send_weights, c, 1, sign))

    with jax.named_scope('hears'):
        for k in range(n - 2):
            hears(k, n - 2 - z, 0, has_dn, -1)
            hears(k, z - 1, 1, has_up, 1)

    local(gate_hbm.at[pl.ds(0, 2)], own, ls_own).wait()
    for m in range(2):
        for c in range(CHUNKS):
            served[m, pl.ds(pl.multiple_of(z * depth, depth), depth), c * fc : (c + 1) * fc] = (
                own[m, :, c * fc : (c + 1) * fc] * gcol
            ).astype(jnp.bfloat16)

    def arrive_all(d):
        for h in range(HALVES):

            def arrive(s, sign):
                tz(s, 0, h).wait_recv()
                nxt = z - sign

                @pl.when((nxt >= 0) & (nxt < n))
                def _():
                    tz(s, -sign, h).start()

                tx(s, h).start()
                tm(s, t, h).start()

            sides(d, arrive)

    def xrelay(s, sign):
        for h in range(HALVES):
            tx(s, h).wait_recv()
            tm(s, xq, h).start()

    def ycopy(c, p, s):
        ref = strip(g, s, c, p)
        return remote(ref, ref, ss_y, rs_y.at[c], grp=1 - g)

    def yforward(c, d, side=None):
        def one(s, sign):
            for p in range(n):
                ref = strip(g, s, c, p)
                remote(ref, ref, ss_w, rs_w.at[c, p, s], fs=s).wait_recv()
                ycopy(c, p, s).start()

        def one_side(s, sign):
            outer = (s == 0) | (s == n - 1)
            pl.when(outer if side == "outer" else jnp.logical_not(outer))(lambda: one(s, sign))

        sides(d, one_side if side else one)

    def ywait(c):
        ref = wsend.at[:, c]
        remote(ref, ref, ss_y, rs_y.at[c], grp=1 - g).wait_recv()

    def hcopy(c, i, to):
        return remote(hs.at[i, c], hr.at[z, c], ss_h, rs_h.at[c], fs=to)

    def sumsq(s):
        part = jnp.zeros((rows, 128), jnp.float32)
        for q in range(nt):
            for i in range(depth // 128):
                x = tok[s * nt + q, :, i * 128 : (i + 1) * 128].astype(jnp.float32)
                part = part + x * x
        total = jnp.sum(part, axis=-1, keepdims=True)
        scale[s] = jnp.broadcast_to(lax.rsqrt(total / width + 1e-06), (rows, fc))

    def compute(c, i):
        rising = i + jnp.where(i >= z, 1, 0)
        falling = n - 1 - i - jnp.where(n - 1 - i <= z, 1, 0)
        s = jnp.where(i == n - 1, z, jnp.where(2 * z >= n, rising, falling))
        strips = pl.ds(pl.multiple_of(c * fc, fc), fc)
        acc = None
        for q in range(nt):
            w = jnp.concatenate(
                [served[m, q * depth : (q + 1) * depth, strips] for m in range(2)], axis=1
            )
            term = jnp.dot(tok[s * nt + q], w, preferred_element_type=jnp.float32)
            acc = term if acc is None else acc + term
        gate = acc[:, :fc] * scale[s]
        up = acc[:, fc:] * scale[s]
        h = (gate / (1.0 + jnp.exp(-gate)) * up).astype(jnp.bfloat16)

        @pl.when(i < n - 1)
        def _():
            hs[i, c] = h
            hcopy(c, i, s).start()

        @pl.when(i == n - 1)
        def _():
            hr[z, c] = h

    inner = jnp.logical_not(at_end)
    late = lax.rem(t, 2) == 1

    def send_far():
        for d in range(2, n):
            for c in range(CHUNKS):
                for sign in (1, -1):
                    s = z + sign * d
                    pl.when((s >= 0) & (s < n))(functools.partial(send_weights, c, d, sign))

    with jax.named_scope("arr1"):
        arrive_all(1)

    local(
        tok_hbm.at[:, pl.ds(0, (nt - 1) * depth)], tok_hbm.at[:, pl.ds(0, (nt - 1) * depth)], ls_tok
    ).wait()
    sumsq(z)

    def rest(s, sign):
        ref = tok.at[pl.ds(0, 2)]
        remote(ref, ref, ss_tok, rs_tm.at[s], tp=mate).wait_recv()
        sumsq(s)

    def totals():
        with jax.named_scope("rest"):
            for d in range(1, n):
                sides(d, rest)

    @pl.when(at_end)
    def _():
        with jax.named_scope("yf0_1"):
            yforward(0, 1)
        with jax.named_scope("xr1"):
            sides(1, xrelay)
        with jax.named_scope("yf1_1"):
            yforward(1, 1)
        for d in range(2, n - 1):
            with jax.named_scope("arr2"):
                arrive_all(d)
        send_far()
        for d in range(2, n - 1):
            with jax.named_scope("xr2"):
                sides(d, xrelay)
        with jax.named_scope("arr3"):
            arrive_all(n - 1)
        with jax.named_scope("yf0_3"):
            yforward(0, n - 1)
        with jax.named_scope("xr3"):
            sides(n - 1, xrelay)
        with jax.named_scope("yf1_3"):
            yforward(1, n - 1)
        totals()
        for c in range(CHUNKS):
            for d in range(2, n - 1):
                with jax.named_scope("yf%d_2" % c):
                    yforward(c, d)

    @pl.when(inner)
    def _():
        for c in range(CHUNKS):
            with jax.named_scope("yf%d_1" % c):
                yforward(c, 1)
        with jax.named_scope("xr1"):
            sides(1, xrelay)
        for d in range(2, n - 1):
            with jax.named_scope("arr2"):
                arrive_all(d)
        for d in range(2, n - 1):
            with jax.named_scope("yf0_2"):
                yforward(0, d)
        send_far()
        for d in range(2, n - 1):
            with jax.named_scope("xr2"):
                sides(d, xrelay)
        for d in range(2, n - 1):
            with jax.named_scope("yf1_2"):
                yforward(1, d)
        totals()

    for copy in small_loads[1:]:
        copy.wait()
    aff = aff_in[...]
    share = aff / jnp.sum(aff, axis=0, keepdims=True)
    top = aff.shape[0]

    def column(row):
        col = jnp.transpose(jnp.broadcast_to(row, (128, rows)))
        return jnp.concatenate([col] * (fc // 128), axis=1) if fc > 128 else col

    shares = [column(share[k : k + 1, :]) for k in range(top)]
    names = [column(names_in[k : k + 1, :].astype(jnp.float32)) for k in range(top)]
    with jax.named_scope("yw0"):
        ywait(0)

    def step(j, carry):
        @pl.when(j == jnp.where(at_end, n - 2, 0))
        def _():
            with jax.named_scope("yw1"):
                ywait(1)

        split = at_end & (j < CHUNKS * (n - 2))
        c = jnp.where(split, j // (n - 2), lax.rem(j, CHUNKS))
        i = jnp.where(split, lax.rem(j, n - 2), j // CHUNKS)
        with jax.named_scope("comp"):
            compute(c, i)
        return carry

    lax.fori_loop(0, n * CHUNKS, step, 0)

    for c in range(CHUNKS):
        ref = hs.at[:, c]
        with jax.named_scope('hw%d' % c):
            remote(ref, ref, ss_h, rs_h.at[c], fs=z).wait_recv()
        picks = []
        for k in range(top):
            picked = jnp.zeros((rows, fc), jnp.float32)
            for e in range(n):
                picked = jnp.where(names[k] == e, hr[e, c].astype(jnp.float32), picked)
            picks.append(picked * shares[k])
        hid_out[:, :, c * fc : (c + 1) * fc] = jnp.stack(picks, axis=1).astype(jnp.bfloat16)

    def sent(ref, sem):
      with jax.named_scope('sent'):
        remote(ref, ref, sem, rs_h.at[0], fs=z).wait_send()

    relayed = 3 * (n - 1)

    @pl.when(at_end)
    def _():
        sent(tok.at[pl.ds(0, relayed + 1)], ss_tok)

    @pl.when(jnp.logical_not(at_end))
    def _():
        sent(tok.at[pl.ds(0, relayed + n + 1)], ss_tok)

    sent(wsend, ss_w)
    sent(wsend, ss_y)
    sent(hs, ss_h)


def emit_kernel(served, hid, gate_out, up_out, hid_out, sems):
    copies = [
        pltpu.make_async_copy(hid, hid_out, sems.at[2]),
        pltpu.make_async_copy(served.at[0], gate_out.at[0], sems.at[0]),
        pltpu.make_async_copy(served.at[1], up_out.at[0], sems.at[1]),
    ]
    for copy in copies:
        copy.start()
    for copy in copies:
        copy.wait()


def dense(tokens, norm_gain, gate_master, up_master, chosen, affinity):
    n, nt = lax.axis_size("fs"), lax.axis_size("tp")
    rows, width = tokens.shape
    experts, depth, fcols = gate_master.shape
    top = chosen.shape[1]
    fc = fcols // CHUNKS
    bf, f32 = jnp.bfloat16, jnp.float32
    dma = pltpu.SemaphoreType.DMA
    hbm = pl.BlockSpec(memory_space=pltpu.HBM)
    vmem = pl.BlockSpec(memory_space=pltpu.VMEM)
    served, hid = pl.pallas_call(
        functools.partial(dense_kernel, n, nt, width),
        out_shape=(
            jax.ShapeDtypeStruct((2, width, fcols), bf),
            jax.ShapeDtypeStruct((rows, top, fcols), bf),
        ),
        in_specs=[hbm] * 6,
        out_specs=(vmem, vmem),
        scratch_shapes=[
            pltpu.VMEM((n * nt, rows, depth), bf),
            pltpu.VMEM((n - 1, depth, fcols), f32),
            pltpu.VMEM((2, depth, fcols), f32),
            pltpu.VMEM((n - 1, CHUNKS, depth, fc), bf),
            pltpu.VMEM((n, rows, fc), f32),
            pltpu.VMEM((n - 1, CHUNKS, rows, fc), bf),
            pltpu.VMEM((n, CHUNKS, rows, fc), bf),
            pltpu.VMEM((1, depth), f32),
            pltpu.VMEM((top, rows), jnp.int32),
            pltpu.VMEM((top, rows), f32),
            dma, dma, dma, dma, dma, dma, dma,
            dma, dma, dma, dma,
            dma((n, HALVES)),
            dma((n, HALVES)),
            dma((n,)),
            dma((CHUNKS, n, n)),
            dma((CHUNKS,)),
            dma((CHUNKS,)),
            pltpu.SemaphoreType.REGULAR((2, n - 2)),
        ],
        compiler_params=pltpu.CompilerParams(
            collective_id=0, has_side_effects=True, vmem_limit_bytes=40 * 1024 * 1024
        ),
    )(*[pltpu.with_memory_space_constraint(x, pltpu.HBM) for x in (tokens, norm_gain.reshape(1, depth), gate_master, up_master, chosen.T, affinity.T)])
    return pl.pallas_call(
        emit_kernel,
        out_shape=(
            jax.ShapeDtypeStruct((1, width, fcols), bf),
            jax.ShapeDtypeStruct((1, width, fcols), bf),
            jax.ShapeDtypeStruct((rows, top, fcols), bf),
        ),
        in_specs=[vmem, vmem],
        out_specs=(hbm, hbm, hbm),
        scratch_shapes=[dma((3,))],
        compiler_params=pltpu.CompilerParams(vmem_limit_bytes=1024 * 1024),
    )(served, hid)


def on_device(tokens, norm_gain, gate_master, up_master, chosen, affinity):
    n, nt = lax.axis_size("fs"), lax.axis_size("tp")
    experts, depth, fcols = gate_master.shape
    rows, width = tokens.shape
    capacity = rows * chosen.shape[1] * 2 // experts
    fits = (
        experts == n
        and capacity >= rows
        and n >= 3
        and nt == 4
        and lax.axis_size("grp") == 2
        and width == nt * depth
        and fcols % (CHUNKS * 128) == 0
        and depth % (16 * n) == 0
    )
    run = dense if fits else routed
    return run(tokens, norm_gain, gate_master, up_master, chosen, affinity)


def solution(mesh):
    return jax.shard_map(
        on_device,
        mesh=mesh,
        in_specs=(
            P(("grp", "fs"), None),
            P("fs"),
            P(None, "fs", "tp"),
            P(None, "fs", "tp"),
            P(("grp", "fs"), None),
            P(("grp", "fs"), None),
        ),
        out_specs=(
            P(("grp", "fs"), None, "tp"),
            P(("grp", "fs"), None, "tp"),
            P(("grp", "fs"), None, "tp"),
        ),
        check_vma=False,
    )
```

```python
import functools

import jax
import jax.numpy as jnp
from jax import lax
from jax.experimental import pallas as pl
from jax.experimental.pallas import tpu as pltpu
from jax.sharding import PartitionSpec as P

MESH = pl.DeviceIdType.MESH
CHUNKS = 2
HALVES = 2


def routed(tokens, norm_gain, gate_master, up_master, chosen, affinity):
    folded_gate = (gate_master * norm_gain[None, :, None]).astype(jnp.bfloat16)
    folded_up = (up_master * norm_gain[None, :, None]).astype(jnp.bfloat16)
    new_gate, new_up = (
        lax.all_to_all(folded_gate, "fs", split_axis=0, concat_axis=1, tiled=True),
        lax.all_to_all(folded_up, "fs", split_axis=0, concat_axis=1, tiled=True),
    )
    experts_all = gate_master.shape[0]
    tok_rows, width = tokens.shape
    top = chosen.shape[1]
    capacity = tok_rows * top * 2 // experts_all
    local = new_gate.shape[0]
    xfloat = tokens.astype(jnp.float32)
    scale = lax.rsqrt(jnp.mean(xfloat * xfloat, axis=-1) + 1e-06)
    share = affinity / jnp.sum(affinity, axis=-1, keepdims=True)
    flat_e = chosen.reshape(-1)
    onehot = (flat_e[:, None] == jnp.arange(experts_all, dtype=jnp.int32)[None, :]).astype(
        jnp.int32
    )
    slot = jnp.sum((jnp.cumsum(onehot, axis=0) - onehot) * onehot, axis=1)
    target = flat_e * capacity + slot
    owner = jnp.repeat(jnp.arange(tok_rows, dtype=jnp.int32), top)
    total = experts_all * capacity
    scale_buf = (
        jnp.zeros((total,), jnp.float32).at[target].set(scale[owner]).reshape(experts_all, capacity)
    )
    share_buf = (
        jnp.zeros((total,), jnp.float32)
        .at[target]
        .set(share.reshape(-1))
        .reshape(experts_all, capacity)
    )
    narrow = width // lax.axis_size("tp")
    own_cols = lax.dynamic_slice_in_dim(tokens, lax.axis_index("tp") * narrow, narrow, 1)
    row_buf = jnp.zeros((total, narrow), jnp.bfloat16).at[target].set(own_cols[owner])
    row_buf = row_buf.reshape(experts_all, capacity, narrow)
    got_rows, got_scale, got_share = (
        lax.all_to_all(row_buf, "fs", split_axis=0, concat_axis=0, tiled=True),
        lax.all_to_all(
            scale_buf.astype(jnp.bfloat16), "fs", split_axis=0, concat_axis=0, tiled=True
        ).astype(scale_buf.dtype),
        lax.all_to_all(
            share_buf.astype(jnp.bfloat16), "fs", split_axis=0, concat_axis=0, tiled=True
        ).astype(share_buf.dtype),
    )
    sources = got_rows.shape[0] // local
    got_rows = got_rows.reshape(sources, local, capacity, narrow)
    piece = lax.all_gather(got_rows, "tp", axis=3, tiled=True)
    gate = jnp.einsum("secd,edf->secf", piece, new_gate, preferred_element_type=jnp.float32)
    up = jnp.einsum("secd,edf->secf", piece, new_up, preferred_element_type=jnp.float32)
    factor = got_scale.reshape(sources, local, capacity)[..., None]
    weight = got_share.reshape(sources, local, capacity)[..., None]
    gate = gate * factor
    up = up * factor
    hidden_rows = (weight * jax.nn.silu(gate) * up).astype(jnp.bfloat16)
    hidden_rows = hidden_rows.reshape(sources * local, capacity, hidden_rows.shape[3])
    back = lax.all_to_all(hidden_rows, "fs", split_axis=0, concat_axis=0, tiled=True)
    picked = back.reshape(total, back.shape[2])[target].reshape(tok_rows, top, back.shape[2])
    return (new_gate, new_up, picked)


def dense_kernel(
    n, nt, width,
    tok_hbm, gain_hbm, gate_hbm, up_hbm, chosen_hbm, aff_hbm,
    served, hr, names, shares,
    tok, wf, own, wsend, scale, hs, gain, names_in, aff_in,
    ls_own_tok, ls_tok, ls_w, ls_own, ls_gain, ls_names, ls_aff,
    ss_tok, ss_w, ss_y, ss_h, rs_tz, rs_tx, rs_tm, rs_w, rs_y, rs_h, far,
):
    g, z, t = lax.axis_index("grp"), lax.axis_index("fs"), lax.axis_index("tp")
    depth, fcols = wf.shape[1], wf.shape[2]
    fc = fcols // CHUNKS
    mate = t + 1 - 2 * lax.rem(t, 2)
    xq = lax.rem(t + 2, nt)
    rows = tok.shape[1]
    has_up, has_dn = z + 1 < n, z > 0
    at_end = (z == 0) | (z == n - 1)

    def remote(src, dst, ssem, rsem, **dev):
        return pltpu.make_async_remote_copy(
            src_ref=src, dst_ref=dst, send_sem=ssem, recv_sem=rsem, device_id=dev, device_id_type=MESH
        )

    def local(src, dst, sem):
        return pltpu.make_async_copy(src, dst, sem)

    def signal(sem, **dev):
        pl.semaphore_signal(sem, 1, device_id=dev, device_id_type=MESH)

    def slot(s):
        return lax.rem(s - z + 2 * n, n) - 1

    barrier = pltpu.get_barrier_semaphore()
    for there, step in ((has_up, 1), (has_dn, -1)):

        @pl.when(there)
        def _():
            signal(barrier, fs=z + step)

    signal(barrier, grp=1 - g)
    signal(barrier, tp=mate)
    signal(barrier, tp=xq)

    def tok_load(q, sem):
        return local(
            tok_hbm.at[:, pl.ds(pl.multiple_of(q * depth, depth), depth)], tok.at[z * nt + q], sem
        )

    own_load = tok_load(t, ls_own_tok)
    own_load.start()
    small_loads = (
        local(gain_hbm, gain, ls_gain),
        local(chosen_hbm, names_in, ls_names),
        local(aff_hbm, aff_in, ls_aff),
    )
    small_loads[0].start()
    for off in range(1, n):
        e = lax.rem(z + off, n)

        @pl.when(g == 0)
        def _():
            local(gate_hbm.at[e], wf.at[off - 1], ls_w).start()

        @pl.when(g != 0)
        def _():
            local(up_hbm.at[e], wf.at[off - 1], ls_w).start()

    for m, ref in enumerate((gate_hbm, up_hbm)):
        local(ref.at[z], own.at[m], ls_own).start()
    for off in range(1, nt):
        tok_load(lax.rem(t + off, nt), ls_tok).start()
    for copy in small_loads[1:]:
        copy.start()

    half = rows // HALVES

    def block(s, q, h):
        return tok.at[s * nt + q, pl.ds(h * half, half)]

    def tz(s, step, h):
        ref = block(s, t, h)
        return remote(ref, ref, ss_tok, rs_tz.at[slot(s - step), h], fs=z + step)

    def tx(s, h):
        ref = block(s, t, h)
        return remote(ref, ref, ss_tok, rs_tx.at[slot(s), h], tp=xq)

    def tm(s, q, h):
        ref = block(s, q, h)
        return remote(ref, ref, ss_tok, rs_tm.at[slot(s)], tp=mate)

    def sides(d, fn):
        for sign in (1, -1):
            s = z + sign * d

            @pl.when((s >= 0) & (s < n))
            def _():
                fn(s, sign)

    with jax.named_scope('tokload'):
        own_load.wait()
    with jax.named_scope('barrier'):
        pl.semaphore_wait(barrier, 5 - jnp.where(at_end, 1, 0))

    for h in range(HALVES):
        sides(1, lambda s, sign: tz(z, sign, h).start())

    @pl.when(has_up & has_dn)
    def _():
        signal(far.at[0, 0], fs=z - 1)
        signal(far.at[1, 0], fs=z + 1)

    with jax.named_scope('gain'):
        small_loads[0].wait()
    gcol = jnp.transpose(jnp.broadcast_to(gain[...], (128, depth)))
    gcol = jnp.concatenate([gcol] * (fc // 128), axis=1) if fc > 128 else gcol
    with jax.named_scope('wload'):
        local(gate_hbm.at[pl.ds(0, n - 1)], wf, ls_w).wait()
    for k in range(n - 1):
        for c in range(CHUNKS):
            wsend[k, c] = (wf[k, :, c * fc : (c + 1) * fc] * gcol).astype(jnp.bfloat16)

    def hears(k, others, way, there, step):
        @pl.when(k < others)
        def _():
            pl.semaphore_wait(far.at[way, k], 1)
            if k + 1 < n - 2:

                @pl.when(there)
                def _():
                    signal(far.at[way, k + 1], fs=z + step)

    def part(s, p):
        size = depth // n
        return pl.ds(pl.multiple_of(s * depth + p * size, size), size)

    def strip(m, s, c, p):
        return served.at[m, part(s, p), pl.ds(c * fc, fc)]

    def wcopy(c, p, to):
        src = wsend.at[slot(to), c, part(0, p)]
        return remote(src, strip(g, z, c, p), ss_w, rs_w.at[c, p, lax.rem(z - to + n, n) - 1], fs=to)

    def send_weights(c, d, sign):
        for p in range(n):
            wcopy(c, p, z + sign * d).start()

    for c in range(CHUNKS):
        for there, sign in ((has_up, 1), (has_dn, -1)):
            outward = at_end | (z + sign == 0) | (z + sign == n - 1)
            now = there if c == 0 else there & outward
            pl.when(now)(functools.partial(send_weights, c, 1, sign))

    def send_to(c, d):
        for sign in (1, -1):
            s = z + sign * d
            pl.when((s >= 0) & (s < n))(functools.partial(send_weights, c, d, sign))

    with jax.named_scope('hears'):
        for k in range(n - 2):
            hears(k, n - 2 - z, 0, has_dn, -1)
            hears(k, z - 1, 1, has_up, 1)

    local(gate_hbm.at[pl.ds(0, 2)], own, ls_own).wait()
    for m in range(2):
        for c in range(CHUNKS):
            served[m, pl.ds(pl.multiple_of(z * depth, depth), depth), c * fc : (c + 1) * fc] = (
                own[m, :, c * fc : (c + 1) * fc] * gcol
            ).astype(jnp.bfloat16)

    def arrive_half(d, h):
        def arrive(s, sign):
            tz(s, 0, h).wait_recv()
            nxt = z - sign

            @pl.when((nxt >= 0) & (nxt < n))
            def _():
                tz(s, -sign, h).start()

            tx(s, h).start()
            tm(s, t, h).start()

        sides(d, arrive)

    def arrive_all(d, between=None):
        for h in range(HALVES):
            if between and h == HALVES - 1:
                between()
            arrive_half(d, h)

    def xrelay(s, sign):
        for h in range(HALVES):
            tx(s, h).wait_recv()
            tm(s, xq, h).start()

    def ycopy(c, p, s):
        ref = strip(g, s, c, p)
        return remote(ref, ref, ss_y, rs_y.at[c], grp=1 - g)

    def yforward(c, d, side=None, piece=None):
        def one(s, sign):
            for p in range(n) if piece is None else (piece,):
                ref = strip(g, s, c, p)
                remote(ref, ref, ss_w, rs_w.at[c, p, slot(s)], fs=s).wait_recv()
                ycopy(c, p, s).start()

        def one_side(s, sign):
            outer = (s == 0) | (s == n - 1)
            pl.when(outer if side == "outer" else jnp.logical_not(outer))(lambda: one(s, sign))

        sides(d, one_side if side else one)

    def ywait(c):
        ref = wsend.at[:, c]
        remote(ref, ref, ss_y, rs_y.at[c], grp=1 - g).wait_recv()

    def hcopy(c, i, to):
        return remote(hs.at[i, c], hr.at[z, c], ss_h, rs_h, fs=to)

    def sumsq(s):
        part = jnp.zeros((rows, 128), jnp.float32)
        for q in range(nt):
            for i in range(depth // 128):
                x = tok[s * nt + q, :, i * 128 : (i + 1) * 128].astype(jnp.float32)
                part = part + x * x
        total = jnp.sum(part, axis=-1, keepdims=True)
        scale[s] = jnp.broadcast_to(lax.rsqrt(total / width + 1e-06), (rows, fc))

    def compute(c, i):
        rising = i + jnp.where(i >= z, 1, 0)
        falling = n - 1 - i - jnp.where(n - 1 - i <= z, 1, 0)
        s = jnp.where(i == n - 1, z, jnp.where(2 * z >= n, rising, falling))
        strips = pl.ds(pl.multiple_of(c * fc, fc), fc)
        acc = None
        for q in range(nt):
            w = jnp.concatenate(
                [served[m, q * depth : (q + 1) * depth, strips] for m in range(2)], axis=1
            )
            term = jnp.dot(tok[s * nt + q], w, preferred_element_type=jnp.float32)
            acc = term if acc is None else acc + term
        gate = acc[:, :fc] * scale[s]
        up = acc[:, fc:] * scale[s]
        h = (gate / (1.0 + jnp.exp(-gate)) * up).astype(jnp.bfloat16)

        @pl.when(i < n - 1)
        def _():
            hs[i, c] = h
            hcopy(c, i, s).start()

        @pl.when(i == n - 1)
        def _():
            hr[z, c] = h

    inner = jnp.logical_not(at_end)
    late = lax.rem(t, 2) == 1

    slow = lax.rem(t, 2) == 0

    def send_far():
        for d in range(2, n):
            for c in range(CHUNKS):
                send_to(c, d)

    def send_mid():
        for d in range(2, n):
            send_to(0, d)
        for sign in (1, -1):
            s = z + sign
            here = (s > 0) & (s < n - 1)
            for c in range(1, CHUNKS):
                pl.when(here)(functools.partial(send_weights, c, 1, sign))

    def send_last():
        for c in range(1, CHUNKS):
            for d in range(2, n):
                send_to(c, d)

    with jax.named_scope("arr1"):
        arrive_all(1)
    pl.when(inner)(send_mid)

    local(
        tok_hbm.at[:, pl.ds(0, (nt - 1) * depth)], tok_hbm.at[:, pl.ds(0, (nt - 1) * depth)], ls_tok
    ).wait()
    sumsq(z)

    def rest(s, sign):
        ref = tok.at[pl.ds(0, 2)]
        remote(ref, ref, ss_tok, rs_tm.at[slot(s)], tp=mate).wait_recv()
        sumsq(s)

    def totals():
        with jax.named_scope("rest"):
            for d in range(1, n):
                sides(d, rest)

    @pl.when(at_end)
    def _():
        with jax.named_scope("yf0_1"):
            yforward(0, 1)
        with jax.named_scope("xr1"):
            sides(1, xrelay)
        with jax.named_scope("yf1_1"):
            yforward(1, 1)
        for d in range(2, n - 1):
            with jax.named_scope("arr2"):
                arrive_all(d, (lambda: pl.when(slow)(send_far)) if d == n - 2 else None)
        pl.when(jnp.logical_not(slow))(send_far)
        for d in range(2, n - 1):
            with jax.named_scope("xr2"):
                sides(d, xrelay)
        for d in range(2, n - 1):
            with jax.named_scope("yf0_2"):
                yforward(0, d)
        with jax.named_scope("arr3a"):
            arrive_half(n - 1, 0)
        for h in range(1, HALVES):
            with jax.named_scope("arr3b"):
                arrive_half(n - 1, h)
        with jax.named_scope("yf0_3"):
            yforward(0, n - 1)
        with jax.named_scope("xr3"):
            sides(n - 1, xrelay)
        with jax.named_scope("yf1_3"):
            yforward(1, n - 1)
        totals()

    @pl.when(inner)
    def _():
        with jax.named_scope("yf0_1"):
            yforward(0, 1)
        with jax.named_scope("yf1_o"):
            yforward(1, 1, "outer")
        with jax.named_scope("xr1"):
            sides(1, xrelay)
        for d in range(2, n - 1):
            with jax.named_scope("arr2"):
                arrive_all(d)
        for d in range(2, n - 1):
            with jax.named_scope("yf0_2"):
                yforward(0, d)
        send_last()
        for d in range(2, n - 1):
            with jax.named_scope("xr2"):
                sides(d, xrelay)
        for d in range(2, n - 1):
            with jax.named_scope("yf1_2"):
                yforward(1, d)
        totals()
        with jax.named_scope("yf1_i"):
            yforward(1, 1, "inner")

    for copy in small_loads[1:]:
        copy.wait()
    aff = aff_in[...]
    share = aff / jnp.sum(aff, axis=0, keepdims=True)

    def column(row):
        col = jnp.transpose(jnp.broadcast_to(row, (128, rows)))
        return jnp.concatenate([col] * (fc // 128), axis=1) if fc > 128 else col

    for k in range(aff.shape[0]):
        shares[k] = column(share[k : k + 1, :])
        names[k] = column(names_in[k : k + 1, :].astype(jnp.float32))
    with jax.named_scope("yw0"):
        ywait(0)

    def step(j, carry):
        with jax.named_scope("yf1_2"):

            @pl.when(at_end & (j < n))
            def _():
                for d in range(2, n - 1):
                    yforward(1, d, piece=j)

        @pl.when(j == n - 1)
        def _():
            with jax.named_scope("yw1"):
                ywait(1)

        split = j < CHUNKS * (n - 1)
        c = jnp.where(split, j // (n - 1), lax.rem(j, CHUNKS))
        i = jnp.where(split, lax.rem(j, n - 1), j // CHUNKS)
        with jax.named_scope("comp"):
            compute(c, i)
        return carry

    lax.fori_loop(0, n * CHUNKS, step, 0)

    with jax.named_scope("hw"):
        remote(hs, hs, ss_h, rs_h, fs=z).wait_recv()

    def sent(ref, sem):
      with jax.named_scope('sent'):
        remote(ref, ref, sem, rs_h, fs=z).wait_send()

    relayed = 3 * (n - 1)

    @pl.when(at_end)
    def _():
        sent(tok.at[pl.ds(0, relayed + 1)], ss_tok)

    @pl.when(jnp.logical_not(at_end))
    def _():
        sent(tok.at[pl.ds(0, relayed + n + 1)], ss_tok)

    sent(wsend, ss_w)
    sent(wsend, ss_y)
    sent(hs, ss_h)


def emit_kernel(served, hr, names, shares, gate_out, up_out, hid_out, hid, sems):
    n, chunks, rows, fc = hr.shape
    copies = [
        pltpu.make_async_copy(served.at[0], gate_out.at[0], sems.at[0]),
        pltpu.make_async_copy(served.at[1], up_out.at[0], sems.at[1]),
    ]
    for copy in copies:
        copy.start()
    for c in range(chunks):
        picks = []
        for k in range(names.shape[0]):
            picked = jnp.zeros((rows, fc), jnp.float32)
            for e in range(n):
                picked = jnp.where(names[k] == e, hr[e, c].astype(jnp.float32), picked)
            picks.append(picked * shares[k])
        hid[c] = jnp.stack(picks, axis=1).astype(jnp.bfloat16)
        copies.append(
            pltpu.make_async_copy(hid.at[c], hid_out.at[:, :, pl.ds(c * fc, fc)], sems.at[2 + c])
        )
        copies[-1].start()
    for copy in copies:
        copy.wait()


def dense(tokens, norm_gain, gate_master, up_master, chosen, affinity):
    n, nt = lax.axis_size("fs"), lax.axis_size("tp")
    rows, width = tokens.shape
    experts, depth, fcols = gate_master.shape
    top = chosen.shape[1]
    fc = fcols // CHUNKS
    bf, f32 = jnp.bfloat16, jnp.float32
    dma = pltpu.SemaphoreType.DMA
    hbm = pl.BlockSpec(memory_space=pltpu.HBM)
    vmem = pl.BlockSpec(memory_space=pltpu.VMEM)
    parts = pl.pallas_call(
        functools.partial(dense_kernel, n, nt, width),
        out_shape=(
            jax.ShapeDtypeStruct((2, width, fcols), bf),
            jax.ShapeDtypeStruct((n, CHUNKS, rows, fc), bf),
            jax.ShapeDtypeStruct((top, rows, fc), f32),
            jax.ShapeDtypeStruct((top, rows, fc), f32),
        ),
        in_specs=[hbm] * 6,
        out_specs=(vmem,) * 4,
        scratch_shapes=[
            pltpu.VMEM((n * nt, rows, depth), bf),
            pltpu.VMEM((n - 1, depth, fcols), f32),
            pltpu.VMEM((2, depth, fcols), f32),
            pltpu.VMEM((n - 1, CHUNKS, depth, fc), bf),
            pltpu.VMEM((n, rows, fc), f32),
            pltpu.VMEM((n - 1, CHUNKS, rows, fc), bf),
            pltpu.VMEM((1, depth), f32),
            pltpu.VMEM((top, rows), jnp.int32),
            pltpu.VMEM((top, rows), f32),
            dma, dma, dma, dma, dma, dma, dma,
            dma, dma, dma, dma,
            dma((n - 1, HALVES)),
            dma((n - 1, HALVES)),
            dma((n - 1,)),
            dma((CHUNKS, n, n - 1)),
            dma((CHUNKS,)),
            dma,
            pltpu.SemaphoreType.REGULAR((2, n - 2)),
        ],
        compiler_params=pltpu.CompilerParams(
            collective_id=0, has_side_effects=True, vmem_limit_bytes=40 * 1024 * 1024
        ),
    )(*[pltpu.with_memory_space_constraint(x, pltpu.HBM) for x in (tokens, norm_gain.reshape(1, depth), gate_master, up_master, chosen.T, affinity.T)])
    return pl.pallas_call(
        emit_kernel,
        out_shape=(
            jax.ShapeDtypeStruct((1, width, fcols), bf),
            jax.ShapeDtypeStruct((1, width, fcols), bf),
            jax.ShapeDtypeStruct((rows, top, fcols), bf),
        ),
        in_specs=[vmem] * 4,
        out_specs=(hbm, hbm, hbm),
        scratch_shapes=[pltpu.VMEM((CHUNKS, rows, top, fc), bf), dma((2 + CHUNKS,))],
        compiler_params=pltpu.CompilerParams(vmem_limit_bytes=1024 * 1024),
    )(*parts)


def on_device(tokens, norm_gain, gate_master, up_master, chosen, affinity):
    n, nt = lax.axis_size("fs"), lax.axis_size("tp")
    experts, depth, fcols = gate_master.shape
    rows, width = tokens.shape
    capacity = rows * chosen.shape[1] * 2 // experts
    fits = (
        experts == n
        and capacity >= rows
        and n >= 3
        and nt == 4
        and lax.axis_size("grp") == 2
        and width == nt * depth
        and fcols % (CHUNKS * 128) == 0
        and depth % (16 * n) == 0
    )
    run = dense if fits else routed
    return run(tokens, norm_gain, gate_master, up_master, chosen, affinity)


def solution(mesh):
    return jax.shard_map(
        on_device,
        mesh=mesh,
        in_specs=(
            P(("grp", "fs"), None),
            P("fs"),
            P(None, "fs", "tp"),
            P(None, "fs", "tp"),
            P(("grp", "fs"), None),
            P(("grp", "fs"), None),
        ),
        out_specs=(
            P(("grp", "fs"), None, "tp"),
            P(("grp", "fs"), None, "tp"),
            P(("grp", "fs"), None, "tp"),
        ),
        check_vma=False,
    )
```

```python
import functools

import jax
import jax.numpy as jnp
from jax import lax
from jax.experimental import pallas as pl
from jax.experimental.pallas import tpu as pltpu
from jax.sharding import PartitionSpec as P

MESH = pl.DeviceIdType.MESH
CHUNKS = 2
HALVES = 2


def routed(tokens, norm_gain, gate_master, up_master, chosen, affinity):
    folded_gate = (gate_master * norm_gain[None, :, None]).astype(jnp.bfloat16)
    folded_up = (up_master * norm_gain[None, :, None]).astype(jnp.bfloat16)
    new_gate, new_up = (
        lax.all_to_all(folded_gate, "fs", split_axis=0, concat_axis=1, tiled=True),
        lax.all_to_all(folded_up, "fs", split_axis=0, concat_axis=1, tiled=True),
    )
    experts_all = gate_master.shape[0]
    tok_rows, width = tokens.shape
    top = chosen.shape[1]
    capacity = tok_rows * top * 2 // experts_all
    local = new_gate.shape[0]
    xfloat = tokens.astype(jnp.float32)
    scale = lax.rsqrt(jnp.mean(xfloat * xfloat, axis=-1) + 1e-06)
    share = affinity / jnp.sum(affinity, axis=-1, keepdims=True)
    flat_e = chosen.reshape(-1)
    onehot = (flat_e[:, None] == jnp.arange(experts_all, dtype=jnp.int32)[None, :]).astype(
        jnp.int32
    )
    slot = jnp.sum((jnp.cumsum(onehot, axis=0) - onehot) * onehot, axis=1)
    target = flat_e * capacity + slot
    owner = jnp.repeat(jnp.arange(tok_rows, dtype=jnp.int32), top)
    total = experts_all * capacity
    scale_buf = (
        jnp.zeros((total,), jnp.float32).at[target].set(scale[owner]).reshape(experts_all, capacity)
    )
    share_buf = (
        jnp.zeros((total,), jnp.float32)
        .at[target]
        .set(share.reshape(-1))
        .reshape(experts_all, capacity)
    )
    narrow = width // lax.axis_size("tp")
    own_cols = lax.dynamic_slice_in_dim(tokens, lax.axis_index("tp") * narrow, narrow, 1)
    row_buf = jnp.zeros((total, narrow), jnp.bfloat16).at[target].set(own_cols[owner])
    row_buf = row_buf.reshape(experts_all, capacity, narrow)
    got_rows, got_scale, got_share = (
        lax.all_to_all(row_buf, "fs", split_axis=0, concat_axis=0, tiled=True),
        lax.all_to_all(
            scale_buf.astype(jnp.bfloat16), "fs", split_axis=0, concat_axis=0, tiled=True
        ).astype(scale_buf.dtype),
        lax.all_to_all(
            share_buf.astype(jnp.bfloat16), "fs", split_axis=0, concat_axis=0, tiled=True
        ).astype(share_buf.dtype),
    )
    sources = got_rows.shape[0] // local
    got_rows = got_rows.reshape(sources, local, capacity, narrow)
    piece = lax.all_gather(got_rows, "tp", axis=3, tiled=True)
    gate = jnp.einsum("secd,edf->secf", piece, new_gate, preferred_element_type=jnp.float32)
    up = jnp.einsum("secd,edf->secf", piece, new_up, preferred_element_type=jnp.float32)
    factor = got_scale.reshape(sources, local, capacity)[..., None]
    weight = got_share.reshape(sources, local, capacity)[..., None]
    gate = gate * factor
    up = up * factor
    hidden_rows = (weight * jax.nn.silu(gate) * up).astype(jnp.bfloat16)
    hidden_rows = hidden_rows.reshape(sources * local, capacity, hidden_rows.shape[3])
    back = lax.all_to_all(hidden_rows, "fs", split_axis=0, concat_axis=0, tiled=True)
    picked = back.reshape(total, back.shape[2])[target].reshape(tok_rows, top, back.shape[2])
    return (new_gate, new_up, picked)


def dense_kernel(
    n, nt, width,
    tok_hbm, gain_hbm, gate_hbm, up_hbm, chosen_hbm, aff_hbm,
    served, hr, names, shares,
    tok, wf, own, wsend, scale, hs, gain, names_in, aff_in,
    ls_own_tok, ls_tok, ls_w, ls_own, ls_gain, ls_names, ls_aff,
    ss_tok, ss_w, ss_y, ss_h, rs_tz, rs_tx, rs_tm, rs_w, rs_y, rs_h, far,
):
    g, z, t = lax.axis_index("grp"), lax.axis_index("fs"), lax.axis_index("tp")
    depth, fcols = wf.shape[1], wf.shape[2]
    fc = fcols // CHUNKS
    mate = t + 1 - 2 * lax.rem(t, 2)
    xq = lax.rem(t + 2, nt)
    rows = tok.shape[1]
    has_up, has_dn = z + 1 < n, z > 0
    at_end = (z == 0) | (z == n - 1)

    def remote(src, dst, ssem, rsem, **dev):
        return pltpu.make_async_remote_copy(
            src_ref=src, dst_ref=dst, send_sem=ssem, recv_sem=rsem, device_id=dev, device_id_type=MESH
        )

    def local(src, dst, sem):
        return pltpu.make_async_copy(src, dst, sem)

    def signal(sem, **dev):
        pl.semaphore_signal(sem, 1, device_id=dev, device_id_type=MESH)

    def slot(s):
        return lax.rem(s - z + 2 * n, n) - 1

    barrier = pltpu.get_barrier_semaphore()
    for there, step in ((has_up, 1), (has_dn, -1)):

        @pl.when(there)
        def _():
            signal(barrier, fs=z + step)

    signal(barrier, grp=1 - g)
    signal(barrier, tp=mate)
    signal(barrier, tp=xq)

    def tok_load(q, sem):
        return local(
            tok_hbm.at[:, pl.ds(pl.multiple_of(q * depth, depth), depth)], tok.at[z * nt + q], sem
        )

    own_load = tok_load(t, ls_own_tok)
    own_load.start()
    small_loads = (
        local(gain_hbm, gain, ls_gain),
        local(chosen_hbm, names_in, ls_names),
        local(aff_hbm, aff_in, ls_aff),
    )
    small_loads[0].start()
    for off in range(1, n):
        e = lax.rem(z + off, n)

        @pl.when(g == 0)
        def _():
            local(gate_hbm.at[e], wf.at[off - 1], ls_w).start()

        @pl.when(g != 0)
        def _():
            local(up_hbm.at[e], wf.at[off - 1], ls_w).start()

    for m, ref in enumerate((gate_hbm, up_hbm)):
        local(ref.at[z], own.at[m], ls_own).start()
    for off in range(1, nt):
        tok_load(lax.rem(t + off, nt), ls_tok).start()
    for copy in small_loads[1:]:
        copy.start()

    half = rows // HALVES

    def block(s, q, h):
        return tok.at[s * nt + q, pl.ds(h * half, half)]

    def tz(s, step, h):
        ref = block(s, t, h)
        return remote(ref, ref, ss_tok, rs_tz.at[slot(s - step), h], fs=z + step)

    def tx(s, h):
        ref = block(s, t, h)
        return remote(ref, ref, ss_tok, rs_tx.at[slot(s), h], tp=xq)

    def tm(s, q, h):
        ref = block(s, q, h)
        return remote(ref, ref, ss_tok, rs_tm.at[slot(s)], tp=mate)

    def sides(d, fn):
        for sign in (1, -1):
            s = z + sign * d

            @pl.when((s >= 0) & (s < n))
            def _():
                fn(s, sign)

    with jax.named_scope('tokload'):
        own_load.wait()
    with jax.named_scope('barrier'):
        pl.semaphore_wait(barrier, 5 - jnp.where(at_end, 1, 0))

    for h in range(HALVES):
        sides(1, lambda s, sign: tz(z, sign, h).start())

    @pl.when(has_up & has_dn)
    def _():
        signal(far.at[0, 0], fs=z - 1)
        signal(far.at[1, 0], fs=z + 1)

    with jax.named_scope('gain'):
        small_loads[0].wait()
    gcol = jnp.transpose(jnp.broadcast_to(gain[...], (128, depth)))
    gcol = jnp.concatenate([gcol] * (fc // 128), axis=1) if fc > 128 else gcol
    with jax.named_scope('wload'):
        local(gate_hbm.at[pl.ds(0, n - 1)], wf, ls_w).wait()
    for k in range(n - 1):
        for c in range(CHUNKS):
            wsend[k, c] = (wf[k, :, c * fc : (c + 1) * fc] * gcol).astype(jnp.bfloat16)

    def hears(k, others, way, there, step):
        @pl.when(k < others)
        def _():
            pl.semaphore_wait(far.at[way, k], 1)
            if k + 1 < n - 2:

                @pl.when(there)
                def _():
                    signal(far.at[way, k + 1], fs=z + step)

    def part(s, p):
        size = depth // n
        return pl.ds(pl.multiple_of(s * depth + p * size, size), size)

    def strip(m, s, c, p):
        return served.at[m, part(s, p), pl.ds(c * fc, fc)]

    def wcopy(c, p, to):
        src = wsend.at[slot(to), c, part(0, p)]
        return remote(src, strip(g, z, c, p), ss_w, rs_w.at[c, p, lax.rem(z - to + n, n) - 1], fs=to)

    def send_weights(c, d, sign, pieces=None):
        for p in pieces or range(n):
            wcopy(c, p, z + sign * d).start()

    for c in range(CHUNKS):
        for there, sign in ((has_up, 1), (has_dn, -1)):
            outward = at_end | (z + sign == 0) | (z + sign == n - 1)
            now = there if c == 0 else there & outward
            pl.when(now)(functools.partial(send_weights, c, 1, sign))

    def send_to(c, d, pieces=None):
        for sign in (1, -1):
            s = z + sign * d
            pl.when((s >= 0) & (s < n))(functools.partial(send_weights, c, d, sign, pieces))

    with jax.named_scope('hears'):
        for k in range(n - 2):
            hears(k, n - 2 - z, 0, has_dn, -1)
            hears(k, z - 1, 1, has_up, 1)

    local(gate_hbm.at[pl.ds(0, 2)], own, ls_own).wait()
    for m in range(2):
        for c in range(CHUNKS):
            served[m, pl.ds(pl.multiple_of(z * depth, depth), depth), c * fc : (c + 1) * fc] = (
                own[m, :, c * fc : (c + 1) * fc] * gcol
            ).astype(jnp.bfloat16)

    def arrive_half(d, h):
        def arrive(s, sign):
            tz(s, 0, h).wait_recv()
            nxt = z - sign

            @pl.when((nxt >= 0) & (nxt < n))
            def _():
                tz(s, -sign, h).start()

            tx(s, h).start()
            tm(s, t, h).start()

        sides(d, arrive)

    def arrive_all(d, between=None):
        for h in range(HALVES):
            if between and h == HALVES - 1:
                between()
            arrive_half(d, h)

    def xrelay(s, sign):
        for h in range(HALVES):
            tx(s, h).wait_recv()
            tm(s, xq, h).start()

    def ycopy(c, p, s):
        ref = strip(g, s, c, p)
        return remote(ref, ref, ss_y, rs_y.at[c], grp=1 - g)

    def yforward(c, d, side=None, piece=None):
        def one(s, sign):
            for p in range(n) if piece is None else (piece,):
                ref = strip(g, s, c, p)
                remote(ref, ref, ss_w, rs_w.at[c, p, slot(s)], fs=s).wait_recv()
                ycopy(c, p, s).start()

        def one_side(s, sign):
            outer = (s == 0) | (s == n - 1)
            pl.when(outer if side == "outer" else jnp.logical_not(outer))(lambda: one(s, sign))

        sides(d, one_side if side else one)

    def ywait(c):
        ref = wsend.at[:, c]
        remote(ref, ref, ss_y, rs_y.at[c], grp=1 - g).wait_recv()

    def hcopy(c, i, to):
        return remote(hs.at[i, c], hr.at[z, c], ss_h, rs_h, fs=to)

    def sumsq(s):
        part = jnp.zeros((rows, 128), jnp.float32)
        for q in range(nt):
            for i in range(depth // 128):
                x = tok[s * nt + q, :, i * 128 : (i + 1) * 128].astype(jnp.float32)
                part = part + x * x
        total = jnp.sum(part, axis=-1, keepdims=True)
        scale[s] = jnp.broadcast_to(lax.rsqrt(total / width + 1e-06), (rows, fc))

    def target(i):
        rising = i + jnp.where(i >= z, 1, 0)
        falling = n - 1 - i - jnp.where(n - 1 - i <= z, 1, 0)
        return jnp.where(i == n - 1, z, jnp.where(2 * z >= n, rising, falling))

    def compute(c, i, held):
        s = target(i)
        strips = pl.ds(pl.multiple_of(c * fc, fc), fc)
        acc = None
        for q in range(nt):
            w = jnp.concatenate(
                [served[m, q * depth : (q + 1) * depth, strips] for m in range(2)], axis=1
            )
            term = jnp.dot(tok[s * nt + q], w, preferred_element_type=jnp.float32)
            acc = term if acc is None else acc + term
        gate = acc[:, :fc] * scale[s]
        up = acc[:, fc:] * scale[s]
        h = (gate / (1.0 + jnp.exp(-gate)) * up).astype(jnp.bfloat16)

        @pl.when(i < n - 1)
        def _():
            hs[i, c] = h
            pl.when(jnp.logical_not(held))(lambda: hcopy(c, i, s).start())

        @pl.when(i == n - 1)
        def _():
            hr[z, c] = h

    inner = jnp.logical_not(at_end)
    late = lax.rem(t, 2) == 1

    slow = lax.rem(t, 2) == 0

    def send_far():
        for d in range(2, n):
            for c in range(CHUNKS):
                send_to(c, d)

    def send_mid():
        for d in range(2, n):
            send_to(0, d)
        for sign in (1, -1):
            s = z + sign
            here = (s > 0) & (s < n - 1)
            for c in range(1, CHUNKS):
                pl.when(here)(functools.partial(send_weights, c, 1, sign))

    soon = z == n - 2

    def send_last(pieces):
        for c in range(1, CHUNKS):
            for d in range(2, n):
                send_to(c, d, pieces)

    with jax.named_scope("arr1"):
        arrive_all(1)
    pl.when(inner)(send_mid)
    pl.when(inner & soon)(lambda: send_last(range(1)))

    local(
        tok_hbm.at[:, pl.ds(0, (nt - 1) * depth)], tok_hbm.at[:, pl.ds(0, (nt - 1) * depth)], ls_tok
    ).wait()
    sumsq(z)

    def rest(s, sign):
        ref = tok.at[pl.ds(0, 2)]
        remote(ref, ref, ss_tok, rs_tm.at[slot(s)], tp=mate).wait_recv()
        sumsq(s)

    def totals():
        with jax.named_scope("rest"):
            for d in range(1, n):
                sides(d, rest)

    @pl.when(at_end)
    def _():
        with jax.named_scope("yf0_1"):
            yforward(0, 1)
        with jax.named_scope("xr1"):
            sides(1, xrelay)
        with jax.named_scope("yf1_1"):
            yforward(1, 1)
        for d in range(2, n - 1):
            with jax.named_scope("arr2"):
                arrive_all(d, (lambda: pl.when(slow)(send_far)) if d == n - 2 else None)
        pl.when(jnp.logical_not(slow))(send_far)
        for d in range(2, n - 1):
            with jax.named_scope("xr2"):
                sides(d, xrelay)
        for d in range(2, n - 1):
            with jax.named_scope("yf0_2"):
                yforward(0, d)
        with jax.named_scope("arr3a"):
            arrive_half(n - 1, 0)
        for h in range(1, HALVES):
            with jax.named_scope("arr3b"):
                arrive_half(n - 1, h)
        with jax.named_scope("yf0_3"):
            yforward(0, n - 1)
        with jax.named_scope("xr3"):
            sides(n - 1, xrelay)
        with jax.named_scope("yf1_3"):
            yforward(1, n - 1)
        totals()

    @pl.when(inner)
    def _():
        with jax.named_scope("yf0_1"):
            yforward(0, 1)
        with jax.named_scope("yf1_o"):
            yforward(1, 1, "outer")
        with jax.named_scope("xr1"):
            sides(1, xrelay)
        for d in range(2, n - 1):
            with jax.named_scope("arr2"):
                arrive_all(d)
        for d in range(2, n - 1):
            with jax.named_scope("yf0_2"):
                yforward(0, d)
        send_last(range(1, n))
        pl.when(jnp.logical_not(soon))(lambda: send_last(range(1)))
        for d in range(2, n - 1):
            with jax.named_scope("xr2"):
                sides(d, xrelay)
        for d in range(2, n - 1):
            with jax.named_scope("yf1_2"):
                yforward(1, d)
        totals()
        with jax.named_scope("yf1_i"):
            yforward(1, 1, "inner")

    for copy in small_loads[1:]:
        copy.wait()
    aff = aff_in[...]
    share = aff / jnp.sum(aff, axis=0, keepdims=True)

    def column(row):
        col = jnp.transpose(jnp.broadcast_to(row, (128, rows)))
        return jnp.concatenate([col] * (fc // 128), axis=1) if fc > 128 else col

    for k in range(aff.shape[0]):
        shares[k] = column(share[k : k + 1, :])
        names[k] = column(names_in[k : k + 1, :].astype(jnp.float32))
    with jax.named_scope("yw0"):
        ywait(0)

    def step(j, carry):
        with jax.named_scope("yf1_2"):

            @pl.when(at_end & (j == 0))
            def _():
                for d in range(2, n - 1):
                    yforward(1, d, piece=0)

            @pl.when(at_end & (j < n - 1))
            def _():
                for d in range(2, n - 1):
                    yforward(1, d, piece=j + 1)

        @pl.when(j == n - 1)
        def _():
            with jax.named_scope("yw1"):
                ywait(1)

        split = j < CHUNKS * (n - 1)
        c = jnp.where(split, j // (n - 1), lax.rem(j, CHUNKS))
        i = jnp.where(split, lax.rem(j, n - 1), j // CHUNKS)
        with jax.named_scope("comp"):
            compute(c, i, inner & (j > 0) & (j < n - 1))

        @pl.when(inner & (j == n - 1))
        def _():
            for k in range(1, n - 1):
                hcopy(0, k, target(k)).start()

        return carry

    lax.fori_loop(0, n * CHUNKS, step, 0)

    with jax.named_scope("hw"):
        remote(hs, hs, ss_h, rs_h, fs=z).wait_recv()

    def sent(ref, sem):
      with jax.named_scope('sent'):
        remote(ref, ref, sem, rs_h, fs=z).wait_send()

    relayed = 3 * (n - 1)

    @pl.when(at_end)
    def _():
        sent(tok.at[pl.ds(0, relayed + 1)], ss_tok)

    @pl.when(jnp.logical_not(at_end))
    def _():
        sent(tok.at[pl.ds(0, relayed + n + 1)], ss_tok)

    sent(wsend, ss_w)
    sent(wsend, ss_y)
    sent(hs, ss_h)


def emit_kernel(served, hr, names, shares, gate_out, up_out, hid_out, hid, sems):
    n, chunks, rows, fc = hr.shape
    copies = [
        pltpu.make_async_copy(served.at[0], gate_out.at[0], sems.at[0]),
        pltpu.make_async_copy(served.at[1], up_out.at[0], sems.at[1]),
    ]
    for copy in copies:
        copy.start()
    for c in range(chunks):
        picks = []
        for k in range(names.shape[0]):
            picked = jnp.zeros((rows, fc), jnp.float32)
            for e in range(n):
                picked = jnp.where(names[k] == e, hr[e, c].astype(jnp.float32), picked)
            picks.append(picked * shares[k])
        hid[c] = jnp.stack(picks, axis=1).astype(jnp.bfloat16)
        copies.append(
            pltpu.make_async_copy(hid.at[c], hid_out.at[:, :, pl.ds(c * fc, fc)], sems.at[2 + c])
        )
        copies[-1].start()
    for copy in copies:
        copy.wait()


def dense(tokens, norm_gain, gate_master, up_master, chosen, affinity):
    n, nt = lax.axis_size("fs"), lax.axis_size("tp")
    rows, width = tokens.shape
    experts, depth, fcols = gate_master.shape
    top = chosen.shape[1]
    fc = fcols // CHUNKS
    bf, f32 = jnp.bfloat16, jnp.float32
    dma = pltpu.SemaphoreType.DMA
    hbm = pl.BlockSpec(memory_space=pltpu.HBM)
    vmem = pl.BlockSpec(memory_space=pltpu.VMEM)
    parts = pl.pallas_call(
        functools.partial(dense_kernel, n, nt, width),
        out_shape=(
            jax.ShapeDtypeStruct((2, width, fcols), bf),
            jax.ShapeDtypeStruct((n, CHUNKS, rows, fc), bf),
            jax.ShapeDtypeStruct((top, rows, fc), f32),
            jax.ShapeDtypeStruct((top, rows, fc), f32),
        ),
        in_specs=[hbm] * 6,
        out_specs=(vmem,) * 4,
        scratch_shapes=[
            pltpu.VMEM((n * nt, rows, depth), bf),
            pltpu.VMEM((n - 1, depth, fcols), f32),
            pltpu.VMEM((2, depth, fcols), f32),
            pltpu.VMEM((n - 1, CHUNKS, depth, fc), bf),
            pltpu.VMEM((n, rows, fc), f32),
            pltpu.VMEM((n - 1, CHUNKS, rows, fc), bf),
            pltpu.VMEM((1, depth), f32),
            pltpu.VMEM((top, rows), jnp.int32),
            pltpu.VMEM((top, rows), f32),
            dma, dma, dma, dma, dma, dma, dma,
            dma, dma, dma, dma,
            dma((n - 1, HALVES)),
            dma((n - 1, HALVES)),
            dma((n - 1,)),
            dma((CHUNKS, n, n - 1)),
            dma((CHUNKS,)),
            dma,
            pltpu.SemaphoreType.REGULAR((2, n - 2)),
        ],
        compiler_params=pltpu.CompilerParams(
            collective_id=0, has_side_effects=True, vmem_limit_bytes=40 * 1024 * 1024
        ),
    )(*[pltpu.with_memory_space_constraint(x, pltpu.HBM) for x in (tokens, norm_gain.reshape(1, depth), gate_master, up_master, chosen.T, affinity.T)])
    return pl.pallas_call(
        emit_kernel,
        out_shape=(
            jax.ShapeDtypeStruct((1, width, fcols), bf),
            jax.ShapeDtypeStruct((1, width, fcols), bf),
            jax.ShapeDtypeStruct((rows, top, fcols), bf),
        ),
        in_specs=[vmem] * 4,
        out_specs=(hbm, hbm, hbm),
        scratch_shapes=[pltpu.VMEM((CHUNKS, rows, top, fc), bf), dma((2 + CHUNKS,))],
        compiler_params=pltpu.CompilerParams(vmem_limit_bytes=1024 * 1024),
    )(*parts)


def on_device(tokens, norm_gain, gate_master, up_master, chosen, affinity):
    n, nt = lax.axis_size("fs"), lax.axis_size("tp")
    experts, depth, fcols = gate_master.shape
    rows, width = tokens.shape
    capacity = rows * chosen.shape[1] * 2 // experts
    fits = (
        experts == n
        and capacity >= rows
        and n >= 3
        and nt == 4
        and lax.axis_size("grp") == 2
        and width == nt * depth
        and fcols % (CHUNKS * 128) == 0
        and depth % (16 * n) == 0
    )
    run = dense if fits else routed
    return run(tokens, norm_gain, gate_master, up_master, chosen, affinity)


def solution(mesh):
    return jax.shard_map(
        on_device,
        mesh=mesh,
        in_specs=(
            P(("grp", "fs"), None),
            P("fs"),
            P(None, "fs", "tp"),
            P(None, "fs", "tp"),
            P(("grp", "fs"), None),
            P(("grp", "fs"), None),
        ),
        out_specs=(
            P(("grp", "fs"), None, "tp"),
            P(("grp", "fs"), None, "tp"),
            P(("grp", "fs"), None, "tp"),
        ),
        check_vma=False,
    )
```

```python
import functools

import jax
import jax.numpy as jnp
from jax import lax
from jax.experimental import pallas as pl
from jax.experimental.pallas import tpu as pltpu
from jax.sharding import PartitionSpec as P

MESH = pl.DeviceIdType.MESH
CHUNKS = 2
HALVES = 2


def routed(tokens, norm_gain, gate_master, up_master, chosen, affinity):
    folded_gate = (gate_master * norm_gain[None, :, None]).astype(jnp.bfloat16)
    folded_up = (up_master * norm_gain[None, :, None]).astype(jnp.bfloat16)
    new_gate, new_up = (
        lax.all_to_all(folded_gate, "fs", split_axis=0, concat_axis=1, tiled=True),
        lax.all_to_all(folded_up, "fs", split_axis=0, concat_axis=1, tiled=True),
    )
    experts_all = gate_master.shape[0]
    tok_rows, width = tokens.shape
    top = chosen.shape[1]
    capacity = tok_rows * top * 2 // experts_all
    local = new_gate.shape[0]
    xfloat = tokens.astype(jnp.float32)
    scale = lax.rsqrt(jnp.mean(xfloat * xfloat, axis=-1) + 1e-06)
    share = affinity / jnp.sum(affinity, axis=-1, keepdims=True)
    flat_e = chosen.reshape(-1)
    onehot = (flat_e[:, None] == jnp.arange(experts_all, dtype=jnp.int32)[None, :]).astype(
        jnp.int32
    )
    slot = jnp.sum((jnp.cumsum(onehot, axis=0) - onehot) * onehot, axis=1)
    target = flat_e * capacity + slot
    owner = jnp.repeat(jnp.arange(tok_rows, dtype=jnp.int32), top)
    total = experts_all * capacity
    scale_buf = (
        jnp.zeros((total,), jnp.float32).at[target].set(scale[owner]).reshape(experts_all, capacity)
    )
    share_buf = (
        jnp.zeros((total,), jnp.float32)
        .at[target]
        .set(share.reshape(-1))
        .reshape(experts_all, capacity)
    )
    narrow = width // lax.axis_size("tp")
    own_cols = lax.dynamic_slice_in_dim(tokens, lax.axis_index("tp") * narrow, narrow, 1)
    row_buf = jnp.zeros((total, narrow), jnp.bfloat16).at[target].set(own_cols[owner])
    row_buf = row_buf.reshape(experts_all, capacity, narrow)
    got_rows, got_scale, got_share = (
        lax.all_to_all(row_buf, "fs", split_axis=0, concat_axis=0, tiled=True),
        lax.all_to_all(
            scale_buf.astype(jnp.bfloat16), "fs", split_axis=0, concat_axis=0, tiled=True
        ).astype(scale_buf.dtype),
        lax.all_to_all(
            share_buf.astype(jnp.bfloat16), "fs", split_axis=0, concat_axis=0, tiled=True
        ).astype(share_buf.dtype),
    )
    sources = got_rows.shape[0] // local
    got_rows = got_rows.reshape(sources, local, capacity, narrow)
    piece = lax.all_gather(got_rows, "tp", axis=3, tiled=True)
    gate = jnp.einsum("secd,edf->secf", piece, new_gate, preferred_element_type=jnp.float32)
    up = jnp.einsum("secd,edf->secf", piece, new_up, preferred_element_type=jnp.float32)
    factor = got_scale.reshape(sources, local, capacity)[..., None]
    weight = got_share.reshape(sources, local, capacity)[..., None]
    gate = gate * factor
    up = up * factor
    hidden_rows = (weight * jax.nn.silu(gate) * up).astype(jnp.bfloat16)
    hidden_rows = hidden_rows.reshape(sources * local, capacity, hidden_rows.shape[3])
    back = lax.all_to_all(hidden_rows, "fs", split_axis=0, concat_axis=0, tiled=True)
    picked = back.reshape(total, back.shape[2])[target].reshape(tok_rows, top, back.shape[2])
    return (new_gate, new_up, picked)


def dense_kernel(
    n, nt, width,
    tok_hbm, gain_hbm, gate_hbm, up_hbm, chosen_hbm, aff_hbm,
    served, hr, names, shares,
    tok, wf, own, wsend, scale, hs, gain, names_in, aff_in,
    ls_own_tok, ls_tok, ls_w, ls_own, ls_gain, ls_names, ls_aff,
    ss_tok, ss_w, ss_y, ss_h, rs_tz, rs_tx, rs_tm, rs_w, rs_y, rs_h, far,
):
    g, z, t = lax.axis_index("grp"), lax.axis_index("fs"), lax.axis_index("tp")
    depth, fcols = wf.shape[1], wf.shape[2]
    fc = fcols // CHUNKS
    mate = t + 1 - 2 * lax.rem(t, 2)
    xq = lax.rem(t + 2, nt)
    rows = tok.shape[1]
    has_up, has_dn = z + 1 < n, z > 0
    at_end = (z == 0) | (z == n - 1)

    def remote(src, dst, ssem, rsem, **dev):
        return pltpu.make_async_remote_copy(
            src_ref=src, dst_ref=dst, send_sem=ssem, recv_sem=rsem, device_id=dev, device_id_type=MESH
        )

    def local(src, dst, sem):
        return pltpu.make_async_copy(src, dst, sem)

    def signal(sem, **dev):
        pl.semaphore_signal(sem, 1, device_id=dev, device_id_type=MESH)

    def slot(s):
        return lax.rem(s - z + 2 * n, n) - 1

    barrier = pltpu.get_barrier_semaphore()
    for there, step in ((has_up, 1), (has_dn, -1)):

        @pl.when(there)
        def _():
            signal(barrier, fs=z + step)

    signal(barrier, grp=1 - g)
    signal(barrier, tp=mate)
    signal(barrier, tp=xq)

    def tok_load(q, sem):
        return local(
            tok_hbm.at[:, pl.ds(pl.multiple_of(q * depth, depth), depth)], tok.at[z * nt + q], sem
        )

    own_load = tok_load(t, ls_own_tok)
    own_load.start()
    small_loads = (
        local(gain_hbm, gain, ls_gain),
        local(chosen_hbm, names_in, ls_names),
        local(aff_hbm, aff_in, ls_aff),
    )
    small_loads[0].start()
    for off in range(1, n):
        e = lax.rem(z + off, n)

        @pl.when(g == 0)
        def _():
            local(gate_hbm.at[e], wf.at[off - 1], ls_w).start()

        @pl.when(g != 0)
        def _():
            local(up_hbm.at[e], wf.at[off - 1], ls_w).start()

    for m, ref in enumerate((gate_hbm, up_hbm)):
        local(ref.at[z], own.at[m], ls_own).start()
    for off in range(1, nt):
        tok_load(lax.rem(t + off, nt), ls_tok).start()
    for copy in small_loads[1:]:
        copy.start()

    half = rows // HALVES

    def block(s, q, h):
        return tok.at[s * nt + q, pl.ds(h * half, half)]

    def tz(s, step, h):
        ref = block(s, t, h)
        return remote(ref, ref, ss_tok, rs_tz.at[slot(s - step), h], fs=z + step)

    def tx(s, h):
        ref = block(s, t, h)
        return remote(ref, ref, ss_tok, rs_tx.at[slot(s), h], tp=xq)

    def tm(s, q, h):
        ref = block(s, q, h)
        return remote(ref, ref, ss_tok, rs_tm.at[slot(s)], tp=mate)

    def sides(d, fn):
        for sign in (1, -1):
            s = z + sign * d

            @pl.when((s >= 0) & (s < n))
            def _():
                fn(s, sign)

    with jax.named_scope('tokload'):
        own_load.wait()
    with jax.named_scope('barrier'):
        pl.semaphore_wait(barrier, 5 - jnp.where(at_end, 1, 0))

    for h in range(HALVES):
        sides(1, lambda s, sign: tz(z, sign, h).start())

    @pl.when(has_up & has_dn)
    def _():
        signal(far.at[0, 0], fs=z - 1)
        signal(far.at[1, 0], fs=z + 1)

    with jax.named_scope('gain'):
        small_loads[0].wait()
    gcol = jnp.transpose(jnp.broadcast_to(gain[...], (128, depth)))
    gcol = jnp.concatenate([gcol] * (fc // 128), axis=1) if fc > 128 else gcol
    with jax.named_scope('wload'):
        local(gate_hbm.at[pl.ds(0, n - 1)], wf, ls_w).wait()
    for k in range(n - 1):
        for c in range(CHUNKS):
            wsend[k, c] = (wf[k, :, c * fc : (c + 1) * fc] * gcol).astype(jnp.bfloat16)

    def hears(k, others, way, there, step):
        @pl.when(k < others)
        def _():
            pl.semaphore_wait(far.at[way, k], 1)
            if k + 1 < n - 2:

                @pl.when(there)
                def _():
                    signal(far.at[way, k + 1], fs=z + step)

    def part(s, p):
        size = depth // n
        return pl.ds(pl.multiple_of(s * depth + p * size, size), size)

    def strip(m, s, c, p):
        return served.at[m, part(s, p), pl.ds(c * fc, fc)]

    def wcopy(c, p, to):
        src = wsend.at[slot(to), c, part(0, p)]
        return remote(src, strip(g, z, c, p), ss_w, rs_w.at[c, p, lax.rem(z - to + n, n) - 1], fs=to)

    def send_weights(c, d, sign, pieces=None):
        for p in pieces or range(n):
            wcopy(c, p, z + sign * d).start()

    for c in range(CHUNKS):
        for there, sign in ((has_up, 1), (has_dn, -1)):
            outward = at_end | (z + sign == 0) | (z + sign == n - 1)
            now = there if c == 0 else there & outward
            pl.when(now)(functools.partial(send_weights, c, 1, sign))

    def send_to(c, d, pieces=None):
        for sign in (1, -1):
            s = z + sign * d
            pl.when((s >= 0) & (s < n))(functools.partial(send_weights, c, d, sign, pieces))

    with jax.named_scope('hears'):
        for k in range(n - 2):
            hears(k, n - 2 - z, 0, has_dn, -1)
            hears(k, z - 1, 1, has_up, 1)

    local(gate_hbm.at[pl.ds(0, 2)], own, ls_own).wait()
    for m in range(2):
        for c in range(CHUNKS):
            served[m, pl.ds(pl.multiple_of(z * depth, depth), depth), c * fc : (c + 1) * fc] = (
                own[m, :, c * fc : (c + 1) * fc] * gcol
            ).astype(jnp.bfloat16)

    def arrive_half(d, h):
        def arrive(s, sign):
            tz(s, 0, h).wait_recv()
            nxt = z - sign

            @pl.when((nxt >= 0) & (nxt < n))
            def _():
                tz(s, -sign, h).start()

            tx(s, h).start()
            tm(s, t, h).start()

        sides(d, arrive)

    def arrive_all(d, between=None):
        for h in range(HALVES):
            if between and h == HALVES - 1:
                between()
            arrive_half(d, h)

    def xrelay(s, sign):
        for h in range(HALVES):
            tx(s, h).wait_recv()
            tm(s, xq, h).start()

    def ycopy(c, p, s):
        ref = strip(g, s, c, p)
        return remote(ref, ref, ss_y, rs_y.at[c], grp=1 - g)

    def yforward(c, d, side=None, piece=None):
        def one(s, sign):
            for p in range(n) if piece is None else (piece,):
                ref = strip(g, s, c, p)
                remote(ref, ref, ss_w, rs_w.at[c, p, slot(s)], fs=s).wait_recv()
                ycopy(c, p, s).start()

        def one_side(s, sign):
            outer = (s == 0) | (s == n - 1)
            pl.when(outer if side == "outer" else jnp.logical_not(outer))(lambda: one(s, sign))

        sides(d, one_side if side else one)

    def ywait(c):
        ref = wsend.at[:, c]
        remote(ref, ref, ss_y, rs_y.at[c], grp=1 - g).wait_recv()

    def hcopy(c, i, to):
        return remote(hs.at[i, c], hr.at[z, c], ss_h, rs_h, fs=to)

    def sumsq(s):
        part = jnp.zeros((rows, 128), jnp.float32)
        for q in range(nt):
            for i in range(depth // 128):
                x = tok[s * nt + q, :, i * 128 : (i + 1) * 128].astype(jnp.float32)
                part = part + x * x
        total = jnp.sum(part, axis=-1, keepdims=True)
        scale[s] = jnp.broadcast_to(lax.rsqrt(total / width + 1e-06), (rows, fc))

    def target(i):
        rising = i + jnp.where(i >= z, 1, 0)
        falling = n - 1 - i - jnp.where(n - 1 - i <= z, 1, 0)
        return jnp.where(i == n - 1, z, jnp.where(2 * z >= n, rising, falling))

    def compute(c, i, held):
        s = target(i)
        strips = pl.ds(pl.multiple_of(c * fc, fc), fc)
        acc = None
        for q in range(nt):
            w = jnp.concatenate(
                [served[m, q * depth : (q + 1) * depth, strips] for m in range(2)], axis=1
            )
            term = jnp.dot(tok[s * nt + q], w, preferred_element_type=jnp.float32)
            acc = term if acc is None else acc + term
        gate = acc[:, :fc] * scale[s]
        up = acc[:, fc:] * scale[s]
        h = (gate / (1.0 + jnp.exp(-gate)) * up).astype(jnp.bfloat16)

        @pl.when(i < n - 1)
        def _():
            hs[i, c] = h
            pl.when(jnp.logical_not(held))(lambda: hcopy(c, i, s).start())

        @pl.when(i == n - 1)
        def _():
            hr[z, c] = h

    inner = jnp.logical_not(at_end)
    late = lax.rem(t, 2) == 1

    slow = lax.rem(t, 2) == 0

    def send_far():
        for d in range(2, n):
            for c in range(CHUNKS):
                send_to(c, d)

    def send_mid():
        for d in range(2, n):
            send_to(0, d)
        for sign in (1, -1):
            s = z + sign
            here = (s > 0) & (s < n - 1)
            for c in range(1, CHUNKS):
                pl.when(here)(functools.partial(send_weights, c, 1, sign))

    soon = z == n - 2

    def send_last(pieces):
        for c in range(1, CHUNKS):
            for d in range(2, n):
                send_to(c, d, pieces)

    with jax.named_scope("arr1"):
        arrive_all(1)
    pl.when(inner)(send_mid)
    pl.when(inner & soon)(lambda: send_last(range(1)))

    local(
        tok_hbm.at[:, pl.ds(0, (nt - 1) * depth)], tok_hbm.at[:, pl.ds(0, (nt - 1) * depth)], ls_tok
    ).wait()
    sumsq(z)

    def rest(s, sign):
        ref = tok.at[pl.ds(0, 2)]
        remote(ref, ref, ss_tok, rs_tm.at[slot(s)], tp=mate).wait_recv()
        sumsq(s)

    def totals():
        with jax.named_scope("rest"):
            for d in range(1, n):
                sides(d, rest)

    @pl.when(at_end)
    def _():
        with jax.named_scope("yf0_1"):
            yforward(0, 1)
        with jax.named_scope("xr1"):
            sides(1, xrelay)
        with jax.named_scope("yf1_1"):
            yforward(1, 1)
        for d in range(2, n - 1):
            with jax.named_scope("arr2"):
                arrive_all(d, (lambda: pl.when(slow)(send_far)) if d == n - 2 else None)
        pl.when(jnp.logical_not(slow))(send_far)
        for d in range(2, n - 1):
            with jax.named_scope("yf0_2"):
                yforward(0, d)
        for d in range(2, n - 1):
            with jax.named_scope("xr2"):
                sides(d, xrelay)
        with jax.named_scope("arr3a"):
            arrive_half(n - 1, 0)
        for h in range(1, HALVES):
            with jax.named_scope("arr3b"):
                arrive_half(n - 1, h)
        with jax.named_scope("yf0_3"):
            yforward(0, n - 1)
        with jax.named_scope("yf1_3"):
            yforward(1, n - 1)
        with jax.named_scope("xr3"):
            sides(n - 1, xrelay)
        totals()

    @pl.when(inner)
    def _():
        with jax.named_scope("yf0_1"):
            yforward(0, 1)
        with jax.named_scope("yf1_o"):
            yforward(1, 1, "outer")
        with jax.named_scope("xr1"):
            sides(1, xrelay)
        for d in range(2, n - 1):
            with jax.named_scope("arr2"):
                arrive_all(d)
        for d in range(2, n - 1):
            with jax.named_scope("yf0_2"):
                yforward(0, d)
        send_last(range(1, n))
        pl.when(jnp.logical_not(soon))(lambda: send_last(range(1)))
        for d in range(2, n - 1):
            with jax.named_scope("xr2"):
                sides(d, xrelay)
        for d in range(2, n - 1):
            with jax.named_scope("yf1_2"):
                yforward(1, d)
        totals()
        with jax.named_scope("yf1_i"):
            yforward(1, 1, "inner")

    for copy in small_loads[1:]:
        copy.wait()
    aff = aff_in[...]
    share = aff / jnp.sum(aff, axis=0, keepdims=True)

    def column(row):
        col = jnp.transpose(jnp.broadcast_to(row, (128, rows)))
        return jnp.concatenate([col] * (fc // 128), axis=1) if fc > 128 else col

    for k in range(aff.shape[0]):
        shares[k] = column(share[k : k + 1, :])
        names[k] = column(names_in[k : k + 1, :].astype(jnp.float32))
    with jax.named_scope("yw0"):
        ywait(0)

    def step(j, carry):
        with jax.named_scope("yf1_2"):

            @pl.when(at_end & (j == 0))
            def _():
                for d in range(2, n - 1):
                    yforward(1, d, piece=0)

            @pl.when(at_end & (j < n - 1))
            def _():
                for d in range(2, n - 1):
                    yforward(1, d, piece=j + 1)

        @pl.when(j == n - 1)
        def _():
            with jax.named_scope("yw1"):
                ywait(1)

        split = j < CHUNKS * (n - 1)
        c = jnp.where(split, j // (n - 1), lax.rem(j, CHUNKS))
        i = jnp.where(split, lax.rem(j, n - 1), j // CHUNKS)
        with jax.named_scope("comp"):
            compute(c, i, inner & (j > 0) & (j < n - 1))

        @pl.when(inner & (j == n - 1))
        def _():
            for k in range(1, n - 1):
                hcopy(0, k, target(k)).start()

        return carry

    lax.fori_loop(0, n * CHUNKS, step, 0)

    with jax.named_scope("hw"):
        remote(hs, hs, ss_h, rs_h, fs=z).wait_recv()

    def sent(ref, sem):
      with jax.named_scope('sent'):
        remote(ref, ref, sem, rs_h, fs=z).wait_send()

    relayed = 3 * (n - 1)

    @pl.when(at_end)
    def _():
        sent(tok.at[pl.ds(0, relayed + 1)], ss_tok)

    @pl.when(jnp.logical_not(at_end))
    def _():
        sent(tok.at[pl.ds(0, relayed + n + 1)], ss_tok)

    sent(wsend, ss_w)
    sent(wsend, ss_y)
    sent(hs, ss_h)


def emit_kernel(served, hr, names, shares, gate_out, up_out, hid_out, hid, sems):
    n, chunks, rows, fc = hr.shape
    copies = [
        pltpu.make_async_copy(served.at[0], gate_out.at[0], sems.at[0]),
        pltpu.make_async_copy(served.at[1], up_out.at[0], sems.at[1]),
    ]
    for copy in copies:
        copy.start()
    for c in range(chunks):
        picks = []
        for k in range(names.shape[0]):
            picked = jnp.zeros((rows, fc), jnp.float32)
            for e in range(n):
                picked = jnp.where(names[k] == e, hr[e, c].astype(jnp.float32), picked)
            picks.append(picked * shares[k])
        hid[c] = jnp.stack(picks, axis=1).astype(jnp.bfloat16)
        copies.append(
            pltpu.make_async_copy(hid.at[c], hid_out.at[:, :, pl.ds(c * fc, fc)], sems.at[2 + c])
        )
        copies[-1].start()
    for copy in copies:
        copy.wait()


def dense(tokens, norm_gain, gate_master, up_master, chosen, affinity):
    n, nt = lax.axis_size("fs"), lax.axis_size("tp")
    rows, width = tokens.shape
    experts, depth, fcols = gate_master.shape
    top = chosen.shape[1]
    fc = fcols // CHUNKS
    bf, f32 = jnp.bfloat16, jnp.float32
    dma = pltpu.SemaphoreType.DMA
    hbm = pl.BlockSpec(memory_space=pltpu.HBM)
    vmem = pl.BlockSpec(memory_space=pltpu.VMEM)
    parts = pl.pallas_call(
        functools.partial(dense_kernel, n, nt, width),
        out_shape=(
            jax.ShapeDtypeStruct((2, width, fcols), bf),
            jax.ShapeDtypeStruct((n, CHUNKS, rows, fc), bf),
            jax.ShapeDtypeStruct((top, rows, fc), f32),
            jax.ShapeDtypeStruct((top, rows, fc), f32),
        ),
        in_specs=[hbm] * 6,
        out_specs=(vmem,) * 4,
        scratch_shapes=[
            pltpu.VMEM((n * nt, rows, depth), bf),
            pltpu.VMEM((n - 1, depth, fcols), f32),
            pltpu.VMEM((2, depth, fcols), f32),
            pltpu.VMEM((n - 1, CHUNKS, depth, fc), bf),
            pltpu.VMEM((n, rows, fc), f32),
            pltpu.VMEM((n - 1, CHUNKS, rows, fc), bf),
            pltpu.VMEM((1, depth), f32),
            pltpu.VMEM((top, rows), jnp.int32),
            pltpu.VMEM((top, rows), f32),
            dma, dma, dma, dma, dma, dma, dma,
            dma, dma, dma, dma,
            dma((n - 1, HALVES)),
            dma((n - 1, HALVES)),
            dma((n - 1,)),
            dma((CHUNKS, n, n - 1)),
            dma((CHUNKS,)),
            dma,
            pltpu.SemaphoreType.REGULAR((2, n - 2)),
        ],
        compiler_params=pltpu.CompilerParams(
            collective_id=0, has_side_effects=True, vmem_limit_bytes=40 * 1024 * 1024
        ),
    )(*[pltpu.with_memory_space_constraint(x, pltpu.HBM) for x in (tokens, norm_gain.reshape(1, depth), gate_master, up_master, chosen.T, affinity.T)])
    return pl.pallas_call(
        emit_kernel,
        out_shape=(
            jax.ShapeDtypeStruct((1, width, fcols), bf),
            jax.ShapeDtypeStruct((1, width, fcols), bf),
            jax.ShapeDtypeStruct((rows, top, fcols), bf),
        ),
        in_specs=[vmem] * 4,
        out_specs=(hbm, hbm, hbm),
        scratch_shapes=[pltpu.VMEM((CHUNKS, rows, top, fc), bf), dma((2 + CHUNKS,))],
        compiler_params=pltpu.CompilerParams(vmem_limit_bytes=1024 * 1024),
    )(*parts)


def on_device(tokens, norm_gain, gate_master, up_master, chosen, affinity):
    n, nt = lax.axis_size("fs"), lax.axis_size("tp")
    experts, depth, fcols = gate_master.shape
    rows, width = tokens.shape
    capacity = rows * chosen.shape[1] * 2 // experts
    fits = (
        experts == n
        and capacity >= rows
        and n >= 4
        and nt == 4
        and lax.axis_size("grp") == 2
        and width == nt * depth
        and fcols % (CHUNKS * 128) == 0
        and depth % (16 * n) == 0
    )
    run = dense if fits else routed
    return run(tokens, norm_gain, gate_master, up_master, chosen, affinity)


def solution(mesh):
    return jax.shard_map(
        on_device,
        mesh=mesh,
        in_specs=(
            P(("grp", "fs"), None),
            P("fs"),
            P(None, "fs", "tp"),
            P(None, "fs", "tp"),
            P(("grp", "fs"), None),
            P(("grp", "fs"), None),
        ),
        out_specs=(
            P(("grp", "fs"), None, "tp"),
            P(("grp", "fs"), None, "tp"),
            P(("grp", "fs"), None, "tp"),
        ),
        check_vma=False,
    )
```

```python
import functools

import jax
import jax.numpy as jnp
from jax import lax
from jax.experimental import pallas as pl
from jax.experimental.pallas import tpu as pltpu
from jax.sharding import PartitionSpec as P

MESH = pl.DeviceIdType.MESH
CHUNKS = 2
HALVES = 2


def routed(tokens, norm_gain, gate_master, up_master, chosen, affinity):
    folded_gate = (gate_master * norm_gain[None, :, None]).astype(jnp.bfloat16)
    folded_up = (up_master * norm_gain[None, :, None]).astype(jnp.bfloat16)
    new_gate, new_up = (
        lax.all_to_all(folded_gate, "fs", split_axis=0, concat_axis=1, tiled=True),
        lax.all_to_all(folded_up, "fs", split_axis=0, concat_axis=1, tiled=True),
    )
    experts_all = gate_master.shape[0]
    tok_rows, width = tokens.shape
    top = chosen.shape[1]
    capacity = tok_rows * top * 2 // experts_all
    local = new_gate.shape[0]
    xfloat = tokens.astype(jnp.float32)
    scale = lax.rsqrt(jnp.mean(xfloat * xfloat, axis=-1) + 1e-06)
    share = affinity / jnp.sum(affinity, axis=-1, keepdims=True)
    flat_e = chosen.reshape(-1)
    onehot = (flat_e[:, None] == jnp.arange(experts_all, dtype=jnp.int32)[None, :]).astype(
        jnp.int32
    )
    slot = jnp.sum((jnp.cumsum(onehot, axis=0) - onehot) * onehot, axis=1)
    target = flat_e * capacity + slot
    owner = jnp.repeat(jnp.arange(tok_rows, dtype=jnp.int32), top)
    total = experts_all * capacity
    scale_buf = (
        jnp.zeros((total,), jnp.float32).at[target].set(scale[owner]).reshape(experts_all, capacity)
    )
    share_buf = (
        jnp.zeros((total,), jnp.float32)
        .at[target]
        .set(share.reshape(-1))
        .reshape(experts_all, capacity)
    )
    narrow = width // lax.axis_size("tp")
    own_cols = lax.dynamic_slice_in_dim(tokens, lax.axis_index("tp") * narrow, narrow, 1)
    row_buf = jnp.zeros((total, narrow), jnp.bfloat16).at[target].set(own_cols[owner])
    row_buf = row_buf.reshape(experts_all, capacity, narrow)
    got_rows, got_scale, got_share = (
        lax.all_to_all(row_buf, "fs", split_axis=0, concat_axis=0, tiled=True),
        lax.all_to_all(
            scale_buf.astype(jnp.bfloat16), "fs", split_axis=0, concat_axis=0, tiled=True
        ).astype(scale_buf.dtype),
        lax.all_to_all(
            share_buf.astype(jnp.bfloat16), "fs", split_axis=0, concat_axis=0, tiled=True
        ).astype(share_buf.dtype),
    )
    sources = got_rows.shape[0] // local
    got_rows = got_rows.reshape(sources, local, capacity, narrow)
    piece = lax.all_gather(got_rows, "tp", axis=3, tiled=True)
    gate = jnp.einsum("secd,edf->secf", piece, new_gate, preferred_element_type=jnp.float32)
    up = jnp.einsum("secd,edf->secf", piece, new_up, preferred_element_type=jnp.float32)
    factor = got_scale.reshape(sources, local, capacity)[..., None]
    weight = got_share.reshape(sources, local, capacity)[..., None]
    gate = gate * factor
    up = up * factor
    hidden_rows = (weight * jax.nn.silu(gate) * up).astype(jnp.bfloat16)
    hidden_rows = hidden_rows.reshape(sources * local, capacity, hidden_rows.shape[3])
    back = lax.all_to_all(hidden_rows, "fs", split_axis=0, concat_axis=0, tiled=True)
    picked = back.reshape(total, back.shape[2])[target].reshape(tok_rows, top, back.shape[2])
    return (new_gate, new_up, picked)


def dense_kernel(
    n, nt, width,
    tok_hbm, gain_hbm, gate_hbm, up_hbm, chosen_hbm, aff_hbm,
    served, hr, names, shares,
    tok, wf, own, wsend, scale, hs, gain, names_in, aff_in,
    ls_own_tok, ls_tok, ls_w, ls_own, ls_gain, ls_names, ls_aff,
    ss_tok, ss_w, ss_y, ss_h, rs_tz, rs_tx, rs_tm, rs_w, rs_y, rs_h, far,
):
    g, z, t = lax.axis_index("grp"), lax.axis_index("fs"), lax.axis_index("tp")
    depth, fcols = wf.shape[1], wf.shape[2]
    fc = fcols // CHUNKS
    mate = t + 1 - 2 * lax.rem(t, 2)
    xq = lax.rem(t + 2, nt)
    rows = tok.shape[1]
    has_up, has_dn = z + 1 < n, z > 0
    at_end = (z == 0) | (z == n - 1)

    def remote(src, dst, ssem, rsem, **dev):
        return pltpu.make_async_remote_copy(
            src_ref=src, dst_ref=dst, send_sem=ssem, recv_sem=rsem, device_id=dev, device_id_type=MESH
        )

    def local(src, dst, sem):
        return pltpu.make_async_copy(src, dst, sem)

    def signal(sem, **dev):
        pl.semaphore_signal(sem, 1, device_id=dev, device_id_type=MESH)

    def slot(s):
        return lax.rem(s - z + 2 * n, n) - 1

    barrier = pltpu.get_barrier_semaphore()
    for there, step in ((has_up, 1), (has_dn, -1)):

        @pl.when(there)
        def _():
            signal(barrier, fs=z + step)

    signal(barrier, grp=1 - g)
    signal(barrier, tp=mate)
    signal(barrier, tp=xq)

    def tok_load(q, sem):
        return local(
            tok_hbm.at[:, pl.ds(pl.multiple_of(q * depth, depth), depth)], tok.at[z * nt + q], sem
        )

    own_load = tok_load(t, ls_own_tok)
    own_load.start()
    small_loads = (
        local(gain_hbm, gain, ls_gain),
        local(chosen_hbm, names_in, ls_names),
        local(aff_hbm, aff_in, ls_aff),
    )
    small_loads[0].start()
    for off in range(1, n):
        e = lax.rem(z + off, n)

        @pl.when(g == 0)
        def _():
            local(gate_hbm.at[e], wf.at[off - 1], ls_w).start()

        @pl.when(g != 0)
        def _():
            local(up_hbm.at[e], wf.at[off - 1], ls_w).start()

    for m, ref in enumerate((gate_hbm, up_hbm)):
        local(ref.at[z], own.at[m], ls_own).start()
    for off in range(1, nt):
        tok_load(lax.rem(t + off, nt), ls_tok).start()
    for copy in small_loads[1:]:
        copy.start()

    half = rows // HALVES

    def block(s, q, h):
        return tok.at[s * nt + q, pl.ds(h * half, half)]

    def tz(s, step, h):
        ref = block(s, t, h)
        return remote(ref, ref, ss_tok, rs_tz.at[slot(s - step), h], fs=z + step)

    def tx(s, h):
        ref = block(s, t, h)
        return remote(ref, ref, ss_tok, rs_tx.at[slot(s), h], tp=xq)

    def tm(s, q, h):
        ref = block(s, q, h)
        return remote(ref, ref, ss_tok, rs_tm.at[slot(s)], tp=mate)

    def sides(d, fn):
        for sign in (1, -1):
            s = z + sign * d

            @pl.when((s >= 0) & (s < n))
            def _():
                fn(s, sign)

    with jax.named_scope('tokload'):
        own_load.wait()
    with jax.named_scope('barrier'):
        pl.semaphore_wait(barrier, 5 - jnp.where(at_end, 1, 0))

    for h in range(HALVES):
        sides(1, lambda s, sign: tz(z, sign, h).start())

    @pl.when(has_up & has_dn)
    def _():
        signal(far.at[0, 0], fs=z - 1)
        signal(far.at[1, 0], fs=z + 1)

    with jax.named_scope('gain'):
        small_loads[0].wait()
    gcol = jnp.transpose(jnp.broadcast_to(gain[...], (128, depth)))
    gcol = jnp.concatenate([gcol] * (fc // 128), axis=1) if fc > 128 else gcol
    with jax.named_scope('wload'):
        local(gate_hbm.at[pl.ds(0, n - 1)], wf, ls_w).wait()
    for k in range(n - 1):
        for c in range(CHUNKS):
            wsend[k, c] = (wf[k, :, c * fc : (c + 1) * fc] * gcol).astype(jnp.bfloat16)

    def hears(k, others, way, there, step):
        @pl.when(k < others)
        def _():
            pl.semaphore_wait(far.at[way, k], 1)
            if k + 1 < n - 2:

                @pl.when(there)
                def _():
                    signal(far.at[way, k + 1], fs=z + step)

    def part(s, p):
        size = depth // n
        return pl.ds(pl.multiple_of(s * depth + p * size, size), size)

    def strip(m, s, c, p):
        return served.at[m, part(s, p), pl.ds(c * fc, fc)]

    def wcopy(c, p, to):
        src = wsend.at[slot(to), c, part(0, p)]
        return remote(src, strip(g, z, c, p), ss_w, rs_w.at[c, p, lax.rem(z - to + n, n) - 1], fs=to)

    def send_weights(c, d, sign, pieces=None):
        for p in pieces or range(n):
            wcopy(c, p, z + sign * d).start()

    for c in range(CHUNKS):
        for there, sign in ((has_up, 1), (has_dn, -1)):
            outward = at_end | (z + sign == 0) | (z + sign == n - 1)
            now = there if c == 0 else there & outward
            pl.when(now)(functools.partial(send_weights, c, 1, sign))

    def send_to(c, d, pieces=None):
        for sign in (1, -1):
            s = z + sign * d
            pl.when((s >= 0) & (s < n))(functools.partial(send_weights, c, d, sign, pieces))

    with jax.named_scope('hears'):
        for k in range(n - 2):
            hears(k, n - 2 - z, 0, has_dn, -1)
            hears(k, z - 1, 1, has_up, 1)

    local(gate_hbm.at[pl.ds(0, 2)], own, ls_own).wait()
    for m in range(2):
        for c in range(CHUNKS):
            served[m, pl.ds(pl.multiple_of(z * depth, depth), depth), c * fc : (c + 1) * fc] = (
                own[m, :, c * fc : (c + 1) * fc] * gcol
            ).astype(jnp.bfloat16)

    def arrive_half(d, h):
        def arrive(s, sign):
            tz(s, 0, h).wait_recv()
            nxt = z - sign

            @pl.when((nxt >= 0) & (nxt < n))
            def _():
                tz(s, -sign, h).start()

            tx(s, h).start()
            tm(s, t, h).start()

        sides(d, arrive)

    def arrive_all(d, between=None):
        for h in range(HALVES):
            if between and h == HALVES - 1:
                between()
            arrive_half(d, h)

    def xrelay(s, sign):
        for h in range(HALVES):
            tx(s, h).wait_recv()
            tm(s, xq, h).start()

    def ycopy(c, p, s):
        ref = strip(g, s, c, p)
        return remote(ref, ref, ss_y, rs_y.at[c], grp=1 - g)

    def yforward(c, d, side=None, piece=None):
        def one(s, sign):
            for p in range(n) if piece is None else (piece,):
                ref = strip(g, s, c, p)
                remote(ref, ref, ss_w, rs_w.at[c, p, slot(s)], fs=s).wait_recv()
                ycopy(c, p, s).start()

        def one_side(s, sign):
            outer = (s == 0) | (s == n - 1)
            pl.when(outer if side == "outer" else jnp.logical_not(outer))(lambda: one(s, sign))

        sides(d, one_side if side else one)

    def ywait(c):
        ref = wsend.at[:, c]
        remote(ref, ref, ss_y, rs_y.at[c], grp=1 - g).wait_recv()

    def hcopy(c, i, to):
        return remote(hs.at[i, c], hr.at[z, c], ss_h, rs_h, fs=to)

    def sumsq(s):
        part = jnp.zeros((rows, 128), jnp.float32)
        for q in range(nt):
            for i in range(depth // 128):
                x = tok[s * nt + q, :, i * 128 : (i + 1) * 128].astype(jnp.float32)
                part = part + x * x
        total = jnp.sum(part, axis=-1, keepdims=True)
        scale[s] = jnp.broadcast_to(lax.rsqrt(total / width + 1e-06), (rows, fc))

    def target(i):
        rising = i + jnp.where(i >= z, 1, 0)
        falling = n - 1 - i - jnp.where(n - 1 - i <= z, 1, 0)
        return jnp.where(i == n - 1, z, jnp.where(2 * z >= n, rising, falling))

    def compute(c, i, held):
        s = target(i)
        strips = pl.ds(pl.multiple_of(c * fc, fc), fc)
        acc = None
        for q in range(nt):
            w = jnp.concatenate(
                [served[m, q * depth : (q + 1) * depth, strips] for m in range(2)], axis=1
            )
            term = jnp.dot(tok[s * nt + q], w, preferred_element_type=jnp.float32)
            acc = term if acc is None else acc + term
        gate = acc[:, :fc] * scale[s]
        up = acc[:, fc:] * scale[s]
        h = (gate / (1.0 + jnp.exp(-gate)) * up).astype(jnp.bfloat16)

        @pl.when(i < n - 1)
        def _():
            hs[i, c] = h
            pl.when(jnp.logical_not(held))(lambda: hcopy(c, i, s).start())

        @pl.when(i == n - 1)
        def _():
            hr[z, c] = h

    inner = jnp.logical_not(at_end)
    late = lax.rem(t, 2) == 1

    slow = lax.rem(t, 2) == 0

    def send_far():
        for d in range(2, n):
            for c in range(CHUNKS):
                send_to(c, d)

    def send_mid():
        for d in range(2, n):
            send_to(0, d)
        for sign in (1, -1):
            s = z + sign
            here = (s > 0) & (s < n - 1)
            for c in range(1, CHUNKS):
                pl.when(here)(functools.partial(send_weights, c, 1, sign))

    soon = z == n - 2

    def send_last(pieces):
        for c in range(1, CHUNKS):
            for d in range(2, n):
                send_to(c, d, pieces)

    with jax.named_scope("arr1"):
        arrive_all(1)
    pl.when(inner)(send_mid)
    pl.when(inner & soon)(lambda: send_last(range(1)))

    local(
        tok_hbm.at[:, pl.ds(0, (nt - 1) * depth)], tok_hbm.at[:, pl.ds(0, (nt - 1) * depth)], ls_tok
    ).wait()
    sumsq(z)

    def rest(s, sign):
        ref = tok.at[pl.ds(0, 2)]
        remote(ref, ref, ss_tok, rs_tm.at[slot(s)], tp=mate).wait_recv()
        sumsq(s)

    def totals():
        with jax.named_scope("rest"):
            for d in range(1, n):
                sides(d, rest)

    @pl.when(at_end)
    def _():
        with jax.named_scope("yf0_1"):
            yforward(0, 1)
        with jax.named_scope("xr1"):
            sides(1, xrelay)
        with jax.named_scope("yf1_1"):
            yforward(1, 1)
        for d in range(2, n - 1):
            with jax.named_scope("arr2"):
                arrive_all(d, (lambda: pl.when(slow)(send_far)) if d == n - 2 else None)
        pl.when(jnp.logical_not(slow))(send_far)
        for d in range(2, n - 1):
            with jax.named_scope("xr2"):
                sides(d, xrelay)
        for d in range(2, n - 1):
            with jax.named_scope("yf0_2"):
                yforward(0, d)
        with jax.named_scope("arr3a"):
            arrive_half(n - 1, 0)
        for h in range(1, HALVES):
            with jax.named_scope("arr3b"):
                arrive_half(n - 1, h)
        with jax.named_scope("yf0_3"):
            yforward(0, n - 1)
        with jax.named_scope("xr3"):
            sides(n - 1, xrelay)
        with jax.named_scope("yf1_3"):
            yforward(1, n - 1)
        totals()

    @pl.when(inner)
    def _():
        with jax.named_scope("yf0_1"):
            yforward(0, 1)
        with jax.named_scope("yf1_o"):
            yforward(1, 1, "outer")
        with jax.named_scope("xr1"):
            sides(1, xrelay)
        for d in range(2, n - 1):
            with jax.named_scope("arr2"):
                arrive_all(d)
        for d in range(2, n - 1):
            with jax.named_scope("yf0_2"):
                yforward(0, d)
        send_last(range(1, n))
        pl.when(jnp.logical_not(soon))(lambda: send_last(range(1)))
        for d in range(2, n - 1):
            with jax.named_scope("xr2"):
                sides(d, xrelay)
        for d in range(2, n - 1):
            with jax.named_scope("yf1_2"):
                yforward(1, d)
        totals()
        with jax.named_scope("yf1_i"):
            yforward(1, 1, "inner")

    for copy in small_loads[1:]:
        copy.wait()
    aff = aff_in[...]
    share = aff / jnp.sum(aff, axis=0, keepdims=True)

    def column(row):
        col = jnp.transpose(jnp.broadcast_to(row, (128, rows)))
        return jnp.concatenate([col] * (fc // 128), axis=1) if fc > 128 else col

    for k in range(aff.shape[0]):
        shares[k] = column(share[k : k + 1, :])
        names[k] = column(names_in[k : k + 1, :].astype(jnp.float32))
    with jax.named_scope("yw0"):
        ywait(0)

    def step(j, carry):
        with jax.named_scope("yf1_2"):

            @pl.when(at_end & (j == 0))
            def _():
                for d in range(2, n - 1):
                    yforward(1, d, piece=0)

            @pl.when(at_end & (j < n - 1))
            def _():
                for d in range(2, n - 1):
                    yforward(1, d, piece=j + 1)

        @pl.when(j == n - 1)
        def _():
            with jax.named_scope("yw1"):
                ywait(1)

        split = j < CHUNKS * (n - 1)
        c = jnp.where(split, j // (n - 1), lax.rem(j, CHUNKS))
        i = jnp.where(split, lax.rem(j, n - 1), j // CHUNKS)
        with jax.named_scope("comp"):
            compute(c, i, inner & (j > 0) & (j < n - 1))

        @pl.when(inner & (j == n - 1))
        def _():
            for k in range(1, n - 1):
                hcopy(0, k, target(k)).start()

        return carry

    lax.fori_loop(0, n * CHUNKS, step, 0)

    with jax.named_scope("hw"):
        remote(hs, hs, ss_h, rs_h, fs=z).wait_recv()

    def sent(ref, sem):
      with jax.named_scope('sent'):
        remote(ref, ref, sem, rs_h, fs=z).wait_send()

    relayed = 3 * (n - 1)

    @pl.when(at_end)
    def _():
        sent(tok.at[pl.ds(0, relayed + 1)], ss_tok)

    @pl.when(jnp.logical_not(at_end))
    def _():
        sent(tok.at[pl.ds(0, relayed + n + 1)], ss_tok)

    sent(wsend, ss_w)
    sent(wsend, ss_y)
    sent(hs, ss_h)


def emit_kernel(served, hr, names, shares, gate_out, up_out, hid_out, hid, sems):
    n, chunks, rows, fc = hr.shape
    copies = [
        pltpu.make_async_copy(served.at[0], gate_out.at[0], sems.at[0]),
        pltpu.make_async_copy(served.at[1], up_out.at[0], sems.at[1]),
    ]
    for copy in copies:
        copy.start()
    for c in range(chunks):
        picks = []
        for k in range(names.shape[0]):
            picked = jnp.zeros((rows, fc), jnp.float32)
            for e in range(n):
                picked = jnp.where(names[k] == e, hr[e, c].astype(jnp.float32), picked)
            picks.append(picked * shares[k])
        hid[c] = jnp.stack(picks, axis=1).astype(jnp.bfloat16)
        copies.append(
            pltpu.make_async_copy(hid.at[c], hid_out.at[:, :, pl.ds(c * fc, fc)], sems.at[2 + c])
        )
        copies[-1].start()
    for copy in copies:
        copy.wait()


def dense(tokens, norm_gain, gate_master, up_master, chosen, affinity):
    n, nt = lax.axis_size("fs"), lax.axis_size("tp")
    rows, width = tokens.shape
    experts, depth, fcols = gate_master.shape
    top = chosen.shape[1]
    fc = fcols // CHUNKS
    bf, f32 = jnp.bfloat16, jnp.float32
    dma = pltpu.SemaphoreType.DMA
    hbm = pl.BlockSpec(memory_space=pltpu.HBM)
    vmem = pl.BlockSpec(memory_space=pltpu.VMEM)
    parts = pl.pallas_call(
        functools.partial(dense_kernel, n, nt, width),
        out_shape=(
            jax.ShapeDtypeStruct((2, width, fcols), bf),
            jax.ShapeDtypeStruct((n, CHUNKS, rows, fc), bf),
            jax.ShapeDtypeStruct((top, rows, fc), f32),
            jax.ShapeDtypeStruct((top, rows, fc), f32),
        ),
        in_specs=[hbm] * 6,
        out_specs=(vmem,) * 4,
        scratch_shapes=[
            pltpu.VMEM((n * nt, rows, depth), bf),
            pltpu.VMEM((n - 1, depth, fcols), f32),
            pltpu.VMEM((2, depth, fcols), f32),
            pltpu.VMEM((n - 1, CHUNKS, depth, fc), bf),
            pltpu.VMEM((n, rows, fc), f32),
            pltpu.VMEM((n - 1, CHUNKS, rows, fc), bf),
            pltpu.VMEM((1, depth), f32),
            pltpu.VMEM((top, rows), jnp.int32),
            pltpu.VMEM((top, rows), f32),
            dma, dma, dma, dma, dma, dma, dma,
            dma, dma, dma, dma,
            dma((n - 1, HALVES)),
            dma((n - 1, HALVES)),
            dma((n - 1,)),
            dma((CHUNKS, n, n - 1)),
            dma((CHUNKS,)),
            dma,
            pltpu.SemaphoreType.REGULAR((2, n - 2)),
        ],
        compiler_params=pltpu.CompilerParams(
            collective_id=0, has_side_effects=True, vmem_limit_bytes=40 * 1024 * 1024
        ),
    )(*[pltpu.with_memory_space_constraint(x, pltpu.HBM) for x in (tokens, norm_gain.reshape(1, depth), gate_master, up_master, chosen.T, affinity.T)])
    return pl.pallas_call(
        emit_kernel,
        out_shape=(
            jax.ShapeDtypeStruct((1, width, fcols), bf),
            jax.ShapeDtypeStruct((1, width, fcols), bf),
            jax.ShapeDtypeStruct((rows, top, fcols), bf),
        ),
        in_specs=[vmem] * 4,
        out_specs=(hbm, hbm, hbm),
        scratch_shapes=[pltpu.VMEM((CHUNKS, rows, top, fc), bf), dma((2 + CHUNKS,))],
        compiler_params=pltpu.CompilerParams(vmem_limit_bytes=1024 * 1024),
    )(*parts)


def on_device(tokens, norm_gain, gate_master, up_master, chosen, affinity):
    n, nt = lax.axis_size("fs"), lax.axis_size("tp")
    experts, depth, fcols = gate_master.shape
    rows, width = tokens.shape
    capacity = rows * chosen.shape[1] * 2 // experts
    fits = (
        experts == n
        and capacity >= rows
        and n >= 4
        and nt == 4
        and lax.axis_size("grp") == 2
        and width == nt * depth
        and fcols % (CHUNKS * 128) == 0
        and depth % (16 * n) == 0
    )
    run = dense if fits else routed
    return run(tokens, norm_gain, gate_master, up_master, chosen, affinity)


def solution(mesh):
    return jax.shard_map(
        on_device,
        mesh=mesh,
        in_specs=(
            P(("grp", "fs"), None),
            P("fs"),
            P(None, "fs", "tp"),
            P(None, "fs", "tp"),
            P(("grp", "fs"), None),
            P(("grp", "fs"), None),
        ),
        out_specs=(
            P(("grp", "fs"), None, "tp"),
            P(("grp", "fs"), None, "tp"),
            P(("grp", "fs"), None, "tp"),
        ),
        check_vma=False,
    )
```

```python
import functools

import jax
import jax.numpy as jnp
from jax import lax
from jax.experimental import pallas as pl
from jax.experimental.pallas import tpu as pltpu
from jax.sharding import PartitionSpec as P

MESH = pl.DeviceIdType.MESH
CHUNKS = 2
HALVES = 2


def routed(tokens, norm_gain, gate_master, up_master, chosen, affinity):
    folded_gate = (gate_master * norm_gain[None, :, None]).astype(jnp.bfloat16)
    folded_up = (up_master * norm_gain[None, :, None]).astype(jnp.bfloat16)
    new_gate, new_up = (
        lax.all_to_all(folded_gate, "fs", split_axis=0, concat_axis=1, tiled=True),
        lax.all_to_all(folded_up, "fs", split_axis=0, concat_axis=1, tiled=True),
    )
    experts_all = gate_master.shape[0]
    tok_rows, width = tokens.shape
    top = chosen.shape[1]
    capacity = tok_rows * top * 2 // experts_all
    local = new_gate.shape[0]
    xfloat = tokens.astype(jnp.float32)
    scale = lax.rsqrt(jnp.mean(xfloat * xfloat, axis=-1) + 1e-06)
    share = affinity / jnp.sum(affinity, axis=-1, keepdims=True)
    flat_e = chosen.reshape(-1)
    onehot = (flat_e[:, None] == jnp.arange(experts_all, dtype=jnp.int32)[None, :]).astype(
        jnp.int32
    )
    slot = jnp.sum((jnp.cumsum(onehot, axis=0) - onehot) * onehot, axis=1)
    target = flat_e * capacity + slot
    owner = jnp.repeat(jnp.arange(tok_rows, dtype=jnp.int32), top)
    total = experts_all * capacity
    scale_buf = (
        jnp.zeros((total,), jnp.float32).at[target].set(scale[owner]).reshape(experts_all, capacity)
    )
    share_buf = (
        jnp.zeros((total,), jnp.float32)
        .at[target]
        .set(share.reshape(-1))
        .reshape(experts_all, capacity)
    )
    narrow = width // lax.axis_size("tp")
    own_cols = lax.dynamic_slice_in_dim(tokens, lax.axis_index("tp") * narrow, narrow, 1)
    row_buf = jnp.zeros((total, narrow), jnp.bfloat16).at[target].set(own_cols[owner])
    row_buf = row_buf.reshape(experts_all, capacity, narrow)
    got_rows, got_scale, got_share = (
        lax.all_to_all(row_buf, "fs", split_axis=0, concat_axis=0, tiled=True),
        lax.all_to_all(
            scale_buf.astype(jnp.bfloat16), "fs", split_axis=0, concat_axis=0, tiled=True
        ).astype(scale_buf.dtype),
        lax.all_to_all(
            share_buf.astype(jnp.bfloat16), "fs", split_axis=0, concat_axis=0, tiled=True
        ).astype(share_buf.dtype),
    )
    sources = got_rows.shape[0] // local
    got_rows = got_rows.reshape(sources, local, capacity, narrow)
    piece = lax.all_gather(got_rows, "tp", axis=3, tiled=True)
    gate = jnp.einsum("secd,edf->secf", piece, new_gate, preferred_element_type=jnp.float32)
    up = jnp.einsum("secd,edf->secf", piece, new_up, preferred_element_type=jnp.float32)
    factor = got_scale.reshape(sources, local, capacity)[..., None]
    weight = got_share.reshape(sources, local, capacity)[..., None]
    gate = gate * factor
    up = up * factor
    hidden_rows = (weight * jax.nn.silu(gate) * up).astype(jnp.bfloat16)
    hidden_rows = hidden_rows.reshape(sources * local, capacity, hidden_rows.shape[3])
    back = lax.all_to_all(hidden_rows, "fs", split_axis=0, concat_axis=0, tiled=True)
    picked = back.reshape(total, back.shape[2])[target].reshape(tok_rows, top, back.shape[2])
    return (new_gate, new_up, picked)


def dense_kernel(
    n, nt, width,
    tok_hbm, gain_hbm, gate_hbm, up_hbm, chosen_hbm, aff_hbm,
    served, hr, names, shares,
    tok, wf, own, wsend, scale, hs, gain, names_in, aff_in,
    ls_own_tok, ls_tok, ls_w, ls_own, ls_gain, ls_names, ls_aff,
    ss_tok, ss_w, ss_y, ss_h, rs_tz, rs_tx, rs_tm, rs_w, rs_y, rs_h, far,
):
    g, z, t = lax.axis_index("grp"), lax.axis_index("fs"), lax.axis_index("tp")
    depth, fcols = wf.shape[1], wf.shape[2]
    fc = fcols // CHUNKS
    mate = t + 1 - 2 * lax.rem(t, 2)
    xq = lax.rem(t + 2, nt)
    rows = tok.shape[1]
    has_up, has_dn = z + 1 < n, z > 0
    at_end = (z == 0) | (z == n - 1)

    def remote(src, dst, ssem, rsem, **dev):
        return pltpu.make_async_remote_copy(
            src_ref=src, dst_ref=dst, send_sem=ssem, recv_sem=rsem, device_id=dev, device_id_type=MESH
        )

    def local(src, dst, sem):
        return pltpu.make_async_copy(src, dst, sem)

    def signal(sem, **dev):
        pl.semaphore_signal(sem, 1, device_id=dev, device_id_type=MESH)

    def slot(s):
        return lax.rem(s - z + 2 * n, n) - 1

    barrier = pltpu.get_barrier_semaphore()
    for there, step in ((has_up, 1), (has_dn, -1)):

        @pl.when(there)
        def _():
            signal(barrier, fs=z + step)

    signal(barrier, grp=1 - g)
    signal(barrier, tp=mate)
    signal(barrier, tp=xq)

    def tok_load(q, sem):
        return local(
            tok_hbm.at[:, pl.ds(pl.multiple_of(q * depth, depth), depth)], tok.at[z * nt + q], sem
        )

    own_load = tok_load(t, ls_own_tok)
    own_load.start()
    small_loads = (
        local(gain_hbm, gain, ls_gain),
        local(chosen_hbm, names_in, ls_names),
        local(aff_hbm, aff_in, ls_aff),
    )
    small_loads[0].start()
    for off in range(1, n):
        e = lax.rem(z + off, n)

        @pl.when(g == 0)
        def _():
            local(gate_hbm.at[e], wf.at[off - 1], ls_w).start()

        @pl.when(g != 0)
        def _():
            local(up_hbm.at[e], wf.at[off - 1], ls_w).start()

    for m, ref in enumerate((gate_hbm, up_hbm)):
        local(ref.at[z], own.at[m], ls_own).start()
    for off in range(1, nt):
        tok_load(lax.rem(t + off, nt), ls_tok).start()
    for copy in small_loads[1:]:
        copy.start()

    half = rows // HALVES

    def block(s, q, h):
        return tok.at[s * nt + q, pl.ds(h * half, half)]

    def tz(s, step, h):
        ref = block(s, t, h)
        return remote(ref, ref, ss_tok, rs_tz.at[slot(s - step), h], fs=z + step)

    def tx(s, h):
        ref = block(s, t, h)
        return remote(ref, ref, ss_tok, rs_tx.at[slot(s), h], tp=xq)

    def tm(s, q, h):
        ref = block(s, q, h)
        return remote(ref, ref, ss_tok, rs_tm.at[slot(s)], tp=mate)

    def sides(d, fn):
        for sign in (1, -1):
            s = z + sign * d

            @pl.when((s >= 0) & (s < n))
            def _():
                fn(s, sign)

    with jax.named_scope('tokload'):
        own_load.wait()
    with jax.named_scope('barrier'):
        pl.semaphore_wait(barrier, 5 - jnp.where(at_end, 1, 0))

    for h in range(HALVES):
        sides(1, lambda s, sign: tz(z, sign, h).start())

    @pl.when(has_up & has_dn)
    def _():
        signal(far.at[0, 0], fs=z - 1)
        signal(far.at[1, 0], fs=z + 1)

    with jax.named_scope('gain'):
        small_loads[0].wait()
    gcol = jnp.transpose(jnp.broadcast_to(gain[...], (128, depth)))
    gcol = jnp.concatenate([gcol] * (fc // 128), axis=1) if fc > 128 else gcol
    with jax.named_scope('wload'):
        local(gate_hbm.at[pl.ds(0, n - 1)], wf, ls_w).wait()
    for k in range(n - 1):
        for c in range(CHUNKS):
            wsend[k, c] = (wf[k, :, c * fc : (c + 1) * fc] * gcol).astype(jnp.bfloat16)

    def hears(k, others, way, there, step):
        @pl.when(k < others)
        def _():
            pl.semaphore_wait(far.at[way, k], 1)
            if k + 1 < n - 2:

                @pl.when(there)
                def _():
                    signal(far.at[way, k + 1], fs=z + step)

    def part(s, p):
        size = depth // n
        return pl.ds(pl.multiple_of(s * depth + p * size, size), size)

    def strip(m, s, c, p):
        return served.at[m, part(s, p), pl.ds(c * fc, fc)]

    def wcopy(c, p, to):
        src = wsend.at[slot(to), c, part(0, p)]
        return remote(src, strip(g, z, c, p), ss_w, rs_w.at[c, p, lax.rem(z - to + n, n) - 1], fs=to)

    def send_weights(c, d, sign, pieces=None):
        for p in pieces or range(n):
            wcopy(c, p, z + sign * d).start()

    for c in range(CHUNKS):
        for there, sign in ((has_up, 1), (has_dn, -1)):
            outward = at_end | (z + sign == 0) | (z + sign == n - 1)
            now = there if c == 0 else there & outward
            pl.when(now)(functools.partial(send_weights, c, 1, sign))

    def send_to(c, d, pieces=None):
        for sign in (1, -1):
            s = z + sign * d
            pl.when((s >= 0) & (s < n))(functools.partial(send_weights, c, d, sign, pieces))

    with jax.named_scope('hears'):
        for k in range(n - 2):
            hears(k, n - 2 - z, 0, has_dn, -1)
            hears(k, z - 1, 1, has_up, 1)

    local(gate_hbm.at[pl.ds(0, 2)], own, ls_own).wait()
    for m in range(2):
        for c in range(CHUNKS):
            served[m, pl.ds(pl.multiple_of(z * depth, depth), depth), c * fc : (c + 1) * fc] = (
                own[m, :, c * fc : (c + 1) * fc] * gcol
            ).astype(jnp.bfloat16)

    def arrive_half(d, h):
        def arrive(s, sign):
            tz(s, 0, h).wait_recv()
            nxt = z - sign

            @pl.when((nxt >= 0) & (nxt < n))
            def _():
                tz(s, -sign, h).start()

            tx(s, h).start()
            tm(s, t, h).start()

        sides(d, arrive)

    def arrive_all(d, between=None):
        for h in range(HALVES):
            if between and h == HALVES - 1:
                between()
            arrive_half(d, h)

    def xrelay(s, sign):
        for h in range(HALVES):
            tx(s, h).wait_recv()
            tm(s, xq, h).start()

    def ycopy(c, p, s):
        ref = strip(g, s, c, p)
        return remote(ref, ref, ss_y, rs_y.at[c], grp=1 - g)

    def yforward(c, d, side=None, piece=None):
        def one(s, sign):
            for p in range(n) if piece is None else (piece,):
                ref = strip(g, s, c, p)
                remote(ref, ref, ss_w, rs_w.at[c, p, slot(s)], fs=s).wait_recv()
                ycopy(c, p, s).start()

        def one_side(s, sign):
            outer = (s == 0) | (s == n - 1)
            pl.when(outer if side == "outer" else jnp.logical_not(outer))(lambda: one(s, sign))

        sides(d, one_side if side else one)

    def ywait(c):
        ref = wsend.at[:, c]
        remote(ref, ref, ss_y, rs_y.at[c], grp=1 - g).wait_recv()

    def hcopy(c, i, to):
        return remote(hs.at[i, c], hr.at[z, c], ss_h, rs_h, fs=to)

    def sumsq(s):
        part = jnp.zeros((rows, 128), jnp.float32)
        for q in range(nt):
            for i in range(depth // 128):
                x = tok[s * nt + q, :, i * 128 : (i + 1) * 128].astype(jnp.float32)
                part = part + x * x
        total = jnp.sum(part, axis=-1, keepdims=True)
        scale[s] = jnp.broadcast_to(lax.rsqrt(total / width + 1e-06), (rows, fc))

    def target(i):
        rising = i + jnp.where(i >= z, 1, 0)
        falling = n - 1 - i - jnp.where(n - 1 - i <= z, 1, 0)
        return jnp.where(i == n - 1, z, jnp.where(2 * z >= n, rising, falling))

    def compute(c, i, held):
        s = target(i)
        strips = pl.ds(pl.multiple_of(c * fc, fc), fc)
        acc = None
        for q in range(nt):
            w = jnp.concatenate(
                [served[m, q * depth : (q + 1) * depth, strips] for m in range(2)], axis=1
            )
            term = jnp.dot(tok[s * nt + q], w, preferred_element_type=jnp.float32)
            acc = term if acc is None else acc + term
        gate = acc[:, :fc] * scale[s]
        up = acc[:, fc:] * scale[s]
        h = (gate / (1.0 + jnp.exp(-gate)) * up).astype(jnp.bfloat16)

        @pl.when(i < n - 1)
        def _():
            hs[i, c] = h
            pl.when(jnp.logical_not(held))(lambda: hcopy(c, i, s).start())

        @pl.when(i == n - 1)
        def _():
            hr[z, c] = h

    inner = jnp.logical_not(at_end)
    late = lax.rem(t, 2) == 1

    slow = lax.rem(t, 2) == 0

    def send_far():
        for d in range(2, n):
            for c in range(CHUNKS):
                send_to(c, d)

    def send_mid():
        for d in range(2, n):
            send_to(0, d)
        for sign in (1, -1):
            s = z + sign
            here = (s > 0) & (s < n - 1)
            for c in range(1, CHUNKS):
                pl.when(here)(functools.partial(send_weights, c, 1, sign))

    soon = (z == n - 2) & (lax.rem(t, 2) == 1)

    def send_last(pieces):
        for c in range(1, CHUNKS):
            for d in range(2, n):
                send_to(c, d, pieces)

    with jax.named_scope("arr1"):
        arrive_all(1)
    pl.when(inner)(send_mid)
    pl.when(inner & soon)(lambda: send_last(range(2)))

    local(
        tok_hbm.at[:, pl.ds(0, (nt - 1) * depth)], tok_hbm.at[:, pl.ds(0, (nt - 1) * depth)], ls_tok
    ).wait()
    sumsq(z)

    def rest(s, sign):
        ref = tok.at[pl.ds(0, 2)]
        remote(ref, ref, ss_tok, rs_tm.at[slot(s)], tp=mate).wait_recv()
        sumsq(s)

    def totals():
        with jax.named_scope("rest"):
            for d in range(1, n):
                sides(d, rest)

    @pl.when(at_end)
    def _():
        with jax.named_scope("yf0_1"):
            yforward(0, 1)
        with jax.named_scope("xr1"):
            sides(1, xrelay)
        with jax.named_scope("yf1_1"):
            yforward(1, 1)
        for d in range(2, n - 1):
            with jax.named_scope("arr2"):
                arrive_all(d, (lambda: pl.when(slow)(send_far)) if d == n - 2 else None)
        pl.when(jnp.logical_not(slow))(send_far)
        for d in range(2, n - 1):
            with jax.named_scope("xr2"):
                sides(d, xrelay)
        for d in range(2, n - 1):
            with jax.named_scope("yf0_2"):
                yforward(0, d)
        with jax.named_scope("arr3a"):
            arrive_half(n - 1, 0)
        for h in range(1, HALVES):
            with jax.named_scope("arr3b"):
                arrive_half(n - 1, h)
        with jax.named_scope("yf0_3"):
            yforward(0, n - 1)
        with jax.named_scope("xr3"):
            sides(n - 1, xrelay)
        with jax.named_scope("yf1_3"):
            yforward(1, n - 1)
        totals()

    @pl.when(inner)
    def _():
        with jax.named_scope("yf0_1"):
            yforward(0, 1)
        with jax.named_scope("yf1_o"):
            yforward(1, 1, "outer")
        with jax.named_scope("xr1"):
            sides(1, xrelay)
        for d in range(2, n - 1):
            with jax.named_scope("arr2"):
                arrive_all(d)
        for d in range(2, n - 1):
            with jax.named_scope("yf0_2"):
                yforward(0, d)
        send_last(range(2, n))
        pl.when(jnp.logical_not(soon))(lambda: send_last(range(2)))
        for d in range(2, n - 1):
            with jax.named_scope("xr2"):
                sides(d, xrelay)
        for d in range(2, n - 1):
            with jax.named_scope("yf1_2"):
                yforward(1, d)
        totals()
        with jax.named_scope("yf1_i"):
            yforward(1, 1, "inner")

    for copy in small_loads[1:]:
        copy.wait()
    aff = aff_in[...]
    share = aff / jnp.sum(aff, axis=0, keepdims=True)

    def column(row):
        col = jnp.transpose(jnp.broadcast_to(row, (128, rows)))
        return jnp.concatenate([col] * (fc // 128), axis=1) if fc > 128 else col

    for k in range(aff.shape[0]):
        shares[k] = column(share[k : k + 1, :])
        names[k] = column(names_in[k : k + 1, :].astype(jnp.float32))
    with jax.named_scope("yw0"):
        ywait(0)

    def step(j, carry):
        with jax.named_scope("yf1_2"):

            @pl.when(at_end & (j == 0))
            def _():
                for d in range(2, n - 1):
                    yforward(1, d, piece=0)

            @pl.when(at_end & (j < n - 1))
            def _():
                for d in range(2, n - 1):
                    yforward(1, d, piece=j + 1)

        @pl.when(j == n - 1)
        def _():
            with jax.named_scope("yw1"):
                ywait(1)

        split = j < CHUNKS * (n - 1)
        c = jnp.where(split, j // (n - 1), lax.rem(j, CHUNKS))
        i = jnp.where(split, lax.rem(j, n - 1), j // CHUNKS)
        with jax.named_scope("comp"):
            compute(c, i, inner & (j > 0) & (j < n - 1))

        @pl.when(inner & (j == n - 1))
        def _():
            for k in range(1, n - 1):
                hcopy(0, k, target(k)).start()

        return carry

    lax.fori_loop(0, n * CHUNKS, step, 0)

    with jax.named_scope("hw"):
        remote(hs, hs, ss_h, rs_h, fs=z).wait_recv()

    def sent(ref, sem):
      with jax.named_scope('sent'):
        remote(ref, ref, sem, rs_h, fs=z).wait_send()

    relayed = 3 * (n - 1)

    @pl.when(at_end)
    def _():
        sent(tok.at[pl.ds(0, relayed + 1)], ss_tok)

    @pl.when(jnp.logical_not(at_end))
    def _():
        sent(tok.at[pl.ds(0, relayed + n + 1)], ss_tok)

    sent(wsend, ss_w)
    sent(wsend, ss_y)
    sent(hs, ss_h)


def emit_kernel(served, hr, names, shares, gate_out, up_out, hid_out, hid, sems):
    n, chunks, rows, fc = hr.shape
    copies = [
        pltpu.make_async_copy(served.at[0], gate_out.at[0], sems.at[0]),
        pltpu.make_async_copy(served.at[1], up_out.at[0], sems.at[1]),
    ]
    for copy in copies:
        copy.start()
    for c in range(chunks):
        picks = []
        for k in range(names.shape[0]):
            picked = jnp.zeros((rows, fc), jnp.float32)
            for e in range(n):
                picked = jnp.where(names[k] == e, hr[e, c].astype(jnp.float32), picked)
            picks.append(picked * shares[k])
        hid[c] = jnp.stack(picks, axis=1).astype(jnp.bfloat16)
        copies.append(
            pltpu.make_async_copy(hid.at[c], hid_out.at[:, :, pl.ds(c * fc, fc)], sems.at[2 + c])
        )
        copies[-1].start()
    for copy in copies:
        copy.wait()


def dense(tokens, norm_gain, gate_master, up_master, chosen, affinity):
    n, nt = lax.axis_size("fs"), lax.axis_size("tp")
    rows, width = tokens.shape
    experts, depth, fcols = gate_master.shape
    top = chosen.shape[1]
    fc = fcols // CHUNKS
    bf, f32 = jnp.bfloat16, jnp.float32
    dma = pltpu.SemaphoreType.DMA
    hbm = pl.BlockSpec(memory_space=pltpu.HBM)
    vmem = pl.BlockSpec(memory_space=pltpu.VMEM)
    parts = pl.pallas_call(
        functools.partial(dense_kernel, n, nt, width),
        out_shape=(
            jax.ShapeDtypeStruct((2, width, fcols), bf),
            jax.ShapeDtypeStruct((n, CHUNKS, rows, fc), bf),
            jax.ShapeDtypeStruct((top, rows, fc), f32),
            jax.ShapeDtypeStruct((top, rows, fc), f32),
        ),
        in_specs=[hbm] * 6,
        out_specs=(vmem,) * 4,
        scratch_shapes=[
            pltpu.VMEM((n * nt, rows, depth), bf),
            pltpu.VMEM((n - 1, depth, fcols), f32),
            pltpu.VMEM((2, depth, fcols), f32),
            pltpu.VMEM((n - 1, CHUNKS, depth, fc), bf),
            pltpu.VMEM((n, rows, fc), f32),
            pltpu.VMEM((n - 1, CHUNKS, rows, fc), bf),
            pltpu.VMEM((1, depth), f32),
            pltpu.VMEM((top, rows), jnp.int32),
            pltpu.VMEM((top, rows), f32),
            dma, dma, dma, dma, dma, dma, dma,
            dma, dma, dma, dma,
            dma((n - 1, HALVES)),
            dma((n - 1, HALVES)),
            dma((n - 1,)),
            dma((CHUNKS, n, n - 1)),
            dma((CHUNKS,)),
            dma,
            pltpu.SemaphoreType.REGULAR((2, n - 2)),
        ],
        compiler_params=pltpu.CompilerParams(
            collective_id=0, has_side_effects=True, vmem_limit_bytes=40 * 1024 * 1024
        ),
    )(*[pltpu.with_memory_space_constraint(x, pltpu.HBM) for x in (tokens, norm_gain.reshape(1, depth), gate_master, up_master, chosen.T, affinity.T)])
    return pl.pallas_call(
        emit_kernel,
        out_shape=(
            jax.ShapeDtypeStruct((1, width, fcols), bf),
            jax.ShapeDtypeStruct((1, width, fcols), bf),
            jax.ShapeDtypeStruct((rows, top, fcols), bf),
        ),
        in_specs=[vmem] * 4,
        out_specs=(hbm, hbm, hbm),
        scratch_shapes=[pltpu.VMEM((CHUNKS, rows, top, fc), bf), dma((2 + CHUNKS,))],
        compiler_params=pltpu.CompilerParams(vmem_limit_bytes=1024 * 1024),
    )(*parts)


def on_device(tokens, norm_gain, gate_master, up_master, chosen, affinity):
    n, nt = lax.axis_size("fs"), lax.axis_size("tp")
    experts, depth, fcols = gate_master.shape
    rows, width = tokens.shape
    capacity = rows * chosen.shape[1] * 2 // experts
    fits = (
        experts == n
        and capacity >= rows
        and n >= 4
        and nt == 4
        and lax.axis_size("grp") == 2
        and width == nt * depth
        and fcols % (CHUNKS * 128) == 0
        and depth % (16 * n) == 0
    )
    run = dense if fits else routed
    return run(tokens, norm_gain, gate_master, up_master, chosen, affinity)


def solution(mesh):
    return jax.shard_map(
        on_device,
        mesh=mesh,
        in_specs=(
            P(("grp", "fs"), None),
            P("fs"),
            P(None, "fs", "tp"),
            P(None, "fs", "tp"),
            P(("grp", "fs"), None),
            P(("grp", "fs"), None),
        ),
        out_specs=(
            P(("grp", "fs"), None, "tp"),
            P(("grp", "fs"), None, "tp"),
            P(("grp", "fs"), None, "tp"),
        ),
        check_vma=False,
    )
```
